512 devices in a mesh: dp: 4 (over x), kv: 64 (over z, y), tp: 2 (over core).
Axes of the slice: x: 4, y: 8, z: 8, core: 2. Of those that a mesh axis runs over, the one named last changes fastest.
Arguments:
- tokens: bfloat16 [131072, 2048], P(('dp', 'kv')), parts along dimension 0, may hold values from -60 to 60, as said below
- chosen: int32 [2048, 16], P(('dp', 'kv')), parts along dimension 0, may hold values from -1 to 511, as said below
- query_weight: bfloat16 [2048, 1024], P('kv', 'tp'), may hold values from -0.125 to 0.125
- key_matrix: bfloat16 [2048, 128], P('kv', 'tp'), may hold values from -0.125 to 0.125
- value_matrix: bfloat16 [2048, 128], P('kv', 'tp'), may hold values from -0.125 to 0.125
- out_weight: bfloat16 [1024, 2048], P('tp', 'kv'), may hold values from -0.1875 to 0.1875
- out_gain: float32 [2048], replicated, may hold values from 0.1 to 1.9
Outputs:
- mixed_out: bfloat16 [131072, 2048], P(('dp', 'kv', 'tp')), parts along dimension 0
The draws below stay inside these ranges and needn't reach their ends.
There are 4 independent parts, one for each index of `dp`. The reference program is written for one: setup_inputs(seed, part) draws one part's arguments, and reference() takes and returns one part's arrays. A program takes and returns all parts, laid end to end along the dimension named above; an argument that names none is the same for every part. Nothing has to cross between parts.
Inputs may be any that keep to these rules, and one draw needn't show every extreme that they name: tokens are of order one apart from few rows. chosen[g, 0] = g; every other entry of row g is -1 or a block below g, and the entries of a row other than -1 are distinct; the blocks that the rows of one device name on any single other device are at most 2 different ones, and this is reached.
All inputs are finite; a program needn't handle non-finite values.
Results may differ from the reference program's by a relative error of at most 0.012.
The reference program's roundings to bfloat16 on the way count: a program that leaves them out, or rounds other values in their place, can miss the bound.
Values may be sent and summed in bfloat16 or wider, within the bound.
A program may use at most 64 MiB of HBM per device.

```python
import jax
import jax.numpy as jnp
from jax import lax

MODEL_WIDTH = 2048
QUERY_HEADS = 16
KEY_VALUE_HEADS = 2
HEAD_WIDTH = 64
BLOCK_LENGTH = 64
SEL = 16
CAP = 2
SEQ = 32768
BLOCKS_DEV = 8
SEQUENCE_BLOCKS = 512
N_KV = 64


def draw_tokens(key, part):
    base = jax.random.normal(key, (SEQ, MODEL_WIDTH), jnp.float32)
    return jnp.clip(base, -60.0, 60.0).astype(jnp.bfloat16)


def draw_chosen(key, part):
    owners = N_KV
    per_dev = BLOCKS_DEV
    parts_keys = jax.random.split(key, 3)
    requester = jnp.arange(owners, dtype=jnp.int32)[:, None]
    holder = jnp.arange(owners, dtype=jnp.int32)[None, :]
    roll = jax.random.randint(parts_keys[0], (owners, owners), 0, 8)
    favored = (holder == 0) | (holder == requester - 1) | (holder == requester - owners // 2)
    counts = jnp.where(favored | (roll < 2), CAP, jnp.where(roll < 4, 1, 0))
    counts = jnp.where(holder < requester, counts, 0)
    order = jax.random.randint(parts_keys[1], (owners, owners, per_dev), 0, 1 << 20) * 1024 + jnp.arange(per_dev, dtype=jnp.int32)
    _, first = lax.top_k(order, min(CAP, per_dev))
    first = jnp.concatenate([first, jnp.zeros((owners, owners, CAP - first.shape[-1]), jnp.int32)], axis=-1)
    slot_index = jnp.arange(CAP, dtype=jnp.int32)
    counts = jnp.minimum(counts, per_dev)
    remote_ids = (holder[:, :, None] * per_dev + first).reshape(owners, owners * CAP)
    remote_live = (slot_index[None, None, :] < counts[:, :, None]).reshape(owners, owners * CAP)
    remote_tier = jnp.broadcast_to(jnp.where(favored, 2, 1)[:, :, None], (owners, owners, CAP)).reshape(owners, owners * CAP)
    local_pos = jnp.arange(per_dev, dtype=jnp.int32)
    local_ids = jnp.broadcast_to((requester * per_dev + local_pos[None, :])[:, None, :], (owners, per_dev, per_dev))
    local_live = jnp.broadcast_to((local_pos[None, :] < local_pos[:, None])[None], (owners, per_dev, per_dev))
    pad_ids = jnp.zeros((owners, per_dev, SEL), jnp.int32)
    pad_live = jnp.zeros((owners, per_dev, SEL), bool)
    cand_ids = jnp.concatenate([jnp.broadcast_to(remote_ids[:, None, :], (owners, per_dev, owners * CAP)), local_ids, pad_ids], axis=-1)
    cand_live = jnp.concatenate([jnp.broadcast_to(remote_live[:, None, :], (owners, per_dev, owners * CAP)), local_live, pad_live], axis=-1)
    cand_tier = jnp.concatenate([jnp.broadcast_to(remote_tier[:, None, :], (owners, per_dev, owners * CAP)), jnp.ones((owners, per_dev, per_dev), jnp.int32), jnp.zeros((owners, per_dev, SEL), jnp.int32)], axis=-1)
    cand_width = owners * CAP + per_dev + SEL
    cand_index = jnp.arange(cand_width, dtype=jnp.int32)[None, None, :]
    noise = jax.random.randint(parts_keys[2], (owners, per_dev, cand_width), 0, 1 << 17)
    score = jnp.where(cand_live, cand_tier * (1 << 28) + noise * 2048 + cand_index, cand_index)
    _, position = lax.top_k(score, SEL - 1)
    taken = jnp.take_along_axis(cand_ids, position, axis=-1)
    live = jnp.take_along_axis(cand_live, position, axis=-1)
    others = jnp.where(live, taken, -1)
    own_ids = (requester * per_dev + local_pos[None, :])[:, :, None]
    return jnp.concatenate([own_ids, others], axis=-1).reshape(owners * per_dev, SEL).astype(jnp.int32)


def block_scale(key, dims, cuts, smallest, high):
    def one(dim, parts):
        heights = jax.random.uniform(jax.random.fold_in(jax.random.fold_in(key, 6), dim), (parts,), jnp.float32, smallest / len(cuts), high / len(cuts))
        return jnp.repeat(jnp.exp(heights), dims[dim] // parts).reshape((-1,) + (1,) * (len(dims) - dim - 1))

    gain = one(*cuts[0])
    for cut in cuts[1:]:
        gain = gain * one(*cut)
    return gain


def centred(stream_key, shape, spread, reach, shards=(), kind=jnp.bfloat16):
    gain = block_scale(stream_key, shape, shards, -0.22, 0.18) if shards else 1.0
    array = jax.random.normal(stream_key, shape, jnp.float32) * spread * gain
    return jnp.minimum(jnp.maximum(array, -reach), reach).astype(kind)


def setup_inputs(seed: int = 0, part: int = 0) -> dict:
    splits = jax.random.split(jax.random.key(seed), 8)
    own_keys = jax.random.split(jax.random.fold_in(splits[7], part), 8)
    return {
        "tokens": draw_tokens(jax.random.fold_in(jax.random.fold_in(splits[7], part), 71), part),
        "chosen": draw_chosen(jax.random.fold_in(jax.random.fold_in(splits[7], part), 71), part),
        "query_weight": centred(splits[2], (MODEL_WIDTH, QUERY_HEADS * HEAD_WIDTH), MODEL_WIDTH ** -0.5, 0.125, ((0, 64), (1, 2))),
        "key_matrix": centred(splits[3], (MODEL_WIDTH, KEY_VALUE_HEADS * HEAD_WIDTH), MODEL_WIDTH ** -0.5, 0.125, ((0, 64), (1, 2))),
        "value_matrix": centred(splits[4], (MODEL_WIDTH, KEY_VALUE_HEADS * HEAD_WIDTH), MODEL_WIDTH ** -0.5, 0.125, ((0, 64), (1, 2))),
        "out_weight": centred(splits[5], (QUERY_HEADS * HEAD_WIDTH, MODEL_WIDTH), (QUERY_HEADS * HEAD_WIDTH) ** -0.5, 0.1875, ((0, 2), (1, 64))),
        "out_gain": jnp.clip(1.0 + 0.18 * jax.random.normal(splits[6], (MODEL_WIDTH,), jnp.float32), 0.1, 1.9),
    }


def reference(tokens, chosen, query_weight, key_matrix, value_matrix, out_weight, out_gain):
    head_groups = QUERY_HEADS // KEY_VALUE_HEADS
    query_rows = jnp.dot(tokens, query_weight, preferred_element_type=jnp.float32).astype(jnp.bfloat16)
    key_rows = jnp.dot(tokens, key_matrix, preferred_element_type=jnp.float32).astype(jnp.bfloat16)
    value_rows = jnp.dot(tokens, value_matrix, preferred_element_type=jnp.float32).astype(jnp.bfloat16)
    blocked_queries = query_rows.reshape(SEQUENCE_BLOCKS, BLOCK_LENGTH, KEY_VALUE_HEADS, head_groups, HEAD_WIDTH)
    blocked_keys = key_rows.reshape(SEQUENCE_BLOCKS, BLOCK_LENGTH, KEY_VALUE_HEADS, HEAD_WIDTH)
    blocked_values = value_rows.reshape(SEQUENCE_BLOCKS, BLOCK_LENGTH, KEY_VALUE_HEADS, HEAD_WIDTH)
    offsets = jnp.arange(BLOCK_LENGTH, dtype=jnp.int32)
    score_scale = HEAD_WIDTH ** (-0.5)

    def one_block(inputs):
        block, row_ids, index = inputs
        safe_ids = jnp.maximum(row_ids, 0).astype(jnp.int32)
        picked_keys = blocked_keys[safe_ids].astype(jnp.float32)
        picked_values = blocked_values[safe_ids].astype(jnp.float32)
        query_pos = index * BLOCK_LENGTH + offsets
        key_pos = safe_ids[:, None] * BLOCK_LENGTH + offsets[None, :]
        visible = (row_ids >= 0)[None, :, None] & (key_pos[None, :, :] <= query_pos[:, None, None])
        scores = jnp.einsum('qhgd,skhd->hgqsk', block.astype(jnp.float32), picked_keys) * score_scale
        scores = jnp.where(visible[None, None], scores, -1e+30)
        row_max = lax.optimization_barrier(jnp.max(scores, axis=(3, 4), keepdims=True))
        expon = jnp.exp(scores - row_max)
        row_sum = lax.optimization_barrier(jnp.sum(expon, axis=(3, 4), keepdims=True))
        weights_bf = (expon / row_sum).astype(jnp.bfloat16)
        result = jnp.einsum('hgqsk,skhd->qhgd', weights_bf.astype(jnp.float32), picked_values)
        return result.astype(jnp.bfloat16)
    attended = lax.map(one_block, (blocked_queries, chosen, jnp.arange(SEQUENCE_BLOCKS, dtype=jnp.int32)))
    attended = attended.reshape(SEQ, QUERY_HEADS * HEAD_WIDTH)
    mixed = jnp.dot(attended, out_weight, preferred_element_type=jnp.float32)
    normed = mixed * lax.rsqrt(lax.optimization_barrier(jnp.mean(mixed * mixed, axis=-1, keepdims=True)) + 1e-06) * out_gain.astype(jnp.float32)
    return normed.astype(jnp.bfloat16)
```

```python
import functools

import jax
import jax.numpy as jnp
from jax import lax
from jax.experimental import pallas as pl
from jax.experimental.pallas import tpu as pltpu
from jax.sharding import PartitionSpec as P

HEAD_WIDTH = 64
BLOCK_LENGTH = 64
CAP = 2
NEG = -1e30
MESH = pl.DeviceIdType.MESH


def fused_kernel(
    dims,
    placed_ref,
    requests_ref,
    tokens_hbm,
    pair_ref,
    query_ref,
    out_ref,
    gain_ref,
    result_ref,
    tokens,
    pair_all,
    requests_all,
    requests_smem,
    query_all,
    out_all,
    own,
    pool,
    packed,
    queries,
    gathered,
    attended,
    part_mine,
    part_send,
    part_recv,
    tok_sem,
    smem_sem,
    pair_sem,
    request_sem,
    y_sem,
    ring_send,
    ring_recv,
    x_send,
    x_recv,
    block_send,
    block_recv,
    half_sem,
):
    n_dp, n_kv, n_y = dims
    n_z = n_kv // n_y
    dp, kv, tp = lax.axis_index("dp"), lax.axis_index("kv"), lax.axis_index("tp")
    z, y = kv // n_y, lax.rem(kv, n_y)
    depth = pair_ref.shape[0]
    blocks = own.shape[0]
    quarter = query_ref.shape[1] // n_dp

    def remote(src, dst, send, recv, to_dp, to_kv, to_tp):
        return pltpu.make_async_remote_copy(
            src_ref=src,
            dst_ref=dst,
            send_sem=send,
            recv_sem=recv,
            device_id=(to_dp, to_kv, to_tp),
            device_id_type=MESH,
        )

    load_tokens = pltpu.make_async_copy(tokens_hbm, tokens, tok_sem)
    load_tokens.start()

    barrier = pltpu.get_barrier_semaphore()

    def greet(off, carry):
        other = lax.rem(kv + off, n_kv)
        pl.semaphore_signal(barrier, inc=1, device_id=(dp, other, tp), device_id_type=MESH)
        return carry

    lax.fori_loop(1, n_kv, greet, 0)
    for off in range(1, n_dp):
        pl.semaphore_signal(
            barrier, inc=1, device_id=(lax.rem(dp + off, n_dp), kv, tp), device_id_type=MESH
        )
    pl.semaphore_signal(barrier, inc=1, device_id=(dp, kv, 1 - tp), device_id_type=MESH)

    my_rows = pl.ds(pl.multiple_of(kv * depth, depth), depth)
    my_cols = pl.ds(pl.multiple_of(dp * quarter, quarter), quarter)
    pair_all[my_rows, :] = pair_ref[...]
    query_all[my_rows, my_cols] = query_ref[:, my_cols]
    out_all[my_rows, my_cols] = out_ref[:, my_cols]

    pl.semaphore_wait(barrier, n_kv - 1 + n_dp - 1 + 1)

    def send_pair(off, carry):
        other = lax.rem(kv + off, n_kv)
        remote(
            pair_ref, pair_all.at[my_rows, :], pair_sem.at[0], pair_sem.at[1], dp, other, tp
        ).start()
        remote(
            requests_ref.at[pl.ds(other, 1)],
            requests_all.at[pl.ds(kv, 1)],
            request_sem.at[0],
            request_sem.at[1],
            dp,
            other,
            tp,
        ).start()
        return carry

    lax.fori_loop(1, n_kv, send_pair, 0)

    def send_row(off, carry):
        other = z * n_y + lax.rem(y + off, n_y)
        remote(
            query_ref.at[:, my_cols],
            query_all.at[my_rows, my_cols],
            y_sem.at[0],
            y_sem.at[1],
            dp,
            other,
            tp,
        ).start()
        remote(
            out_ref.at[:, my_cols],
            out_all.at[my_rows, my_cols],
            y_sem.at[2],
            y_sem.at[3],
            dp,
            other,
            tp,
        ).start()
        return carry

    lax.fori_loop(1, n_y, send_row, 0)

    def drain(ref, sem):
        pltpu.make_async_copy(ref, ref, sem).wait()

    others = pair_all.at[pl.ds(0, (n_kv - 1) * depth), :]
    drain(others, pair_sem.at[1])
    drain(requests_all.at[pl.ds(0, n_kv - 1)], request_sem.at[1])
    to_smem = pltpu.make_async_copy(requests_all, requests_smem, smem_sem)
    to_smem.start()
    load_tokens.wait()
    pairs = jnp.dot(tokens[...], pair_all[...], preferred_element_type=jnp.float32)
    pairs = pairs.astype(jnp.bfloat16).reshape(own.shape)
    own[...] = pairs
    pool[pl.ds(n_kv * CAP, blocks)] = pairs
    to_smem.wait()

    def block_copy(owner, to):
        return remote(
            packed.at[to],
            pool.at[pl.ds(owner * CAP, CAP)],
            block_send.at[to],
            block_recv.at[owner],
            dp,
            to,
            tp,
        )

    def send_blocks(off, carry):
        to = kv + off

        @pl.when(to < n_kv)
        def _():
            for slot in range(CAP):
                packed[to, slot] = own[requests_smem[to, 0, slot]]
            block_copy(kv, to).start()

        return carry

    lax.fori_loop(1, n_kv, send_blocks, 0)

    row_others = pair_all.at[pl.ds(0, (n_y - 1) * depth), :]
    drain(row_others, y_sem.at[1])
    drain(row_others, y_sem.at[3])

    above = lax.rem(z + 1, n_z) * n_y + y
    below = lax.rem(z + n_z - 1, n_z) * n_y + y
    bundle_depth = n_y * depth

    def bundle(ref, which):
        start = pl.multiple_of(lax.rem(which + n_z, n_z) * bundle_depth, bundle_depth)
        return ref.at[pl.ds(start, bundle_depth), my_cols]

    def ring(step, part, up):
        ref = (query_all, out_all)[part]
        piece = bundle(ref, z - step if up else z + step)
        at = (step * 2 + part) * 2 + (0 if up else 1)
        return remote(
            piece, piece, ring_send.at[at], ring_recv.at[at], dp, above if up else below, tp
        )

    half = n_z // 2
    started = []
    for step in range(half):
        now = []
        if step:
            for copy in started[-1]:
                copy.wait_recv()
        for part in range(2):
            for up in (True, False):
                if step == half - 1 and up != (part == 0):
                    continue
                now.append(ring(step, part, up))
        for copy in now:
            copy.start()
        started.append(now)
    for copy in started[-1]:
        copy.wait_recv()
    for group in started:
        for copy in group:
            copy.wait_send()

    right, left = lax.rem(dp + 1, n_dp), lax.rem(dp + n_dp - 1, n_dp)

    def columns(ref, which):
        start = pl.multiple_of(lax.rem(which + n_dp, n_dp) * quarter, quarter)
        return ref.at[:, pl.ds(start, quarter)]

    def across(at, ref, which, to):
        piece = columns(ref, which)
        return remote(piece, piece, x_send.at[at], x_recv.at[at], to, kv, tp)

    query_right, query_left = across(0, query_all, dp, right), across(1, query_all, dp, left)
    out_right, out_left = across(2, out_all, dp, right), across(3, out_all, dp, left)
    query_on = across(4, query_all, dp - 1, right)
    out_on = across(5, out_all, dp + 1, left)
    query_right.start()
    query_left.start()
    out_left.start()
    query_right.wait_recv()
    query_on.start()
    out_right.start()
    query_left.wait_recv()
    out_left.wait_recv()
    out_on.start()
    query_on.wait_recv()

    lane = lax.broadcasted_iota(jnp.int32, (tokens.shape[0], 2 * HEAD_WIDTH), 1)
    for d in range(n_dp):
        rows = jnp.dot(
            tokens[...],
            query_all[:, d * quarter : (d + 1) * quarter],
            preferred_element_type=jnp.float32,
        )
        rows = rows.astype(jnp.bfloat16).astype(jnp.float32) * HEAD_WIDTH ** (-0.5)
        turned = pltpu.roll(rows, HEAD_WIDTH, 1)
        for side, value in enumerate((rows, turned)):
            head = jnp.where(lane < HEAD_WIDTH, value, 0.0).astype(jnp.bfloat16)
            queries[:, 2 * d + side] = head.reshape(blocks, BLOCK_LENGTH, 2 * HEAD_WIDTH)

    def wait_blocks(owner, carry):
        @pl.when(owner < kv)
        def _():
            block_copy(owner, kv).wait_recv()

        return carry

    lax.fori_loop(0, n_kv, wait_blocks, 0)

    sel = placed_ref.shape[1]
    pair_rows = 2 * BLOCK_LENGTH
    row_at = lax.broadcasted_iota(jnp.int32, (pair_rows, 2 * HEAD_WIDTH), 0)
    lane_at = lax.broadcasted_iota(jnp.int32, (pair_rows, 2 * HEAD_WIDTH), 1)
    first_half = lane_at < BLOCK_LENGTH
    own_bias = jnp.where(lane_at <= lax.rem(row_at, BLOCK_LENGTH), 0.0, NEG)

    def attend(block, carry):
        shut = []
        for s in range(sel):
            at = placed_ref[block, s]
            gathered[s * BLOCK_LENGTH : (s + 1) * BLOCK_LENGTH, :] = pool[jnp.maximum(at, 0)]
            shut.append(jnp.where(at < 0, NEG, 0.0))
        bias = [jnp.where(first_half, own_bias, shut[1])]
        for s in range(2, sel, 2):
            bias.append(jnp.where(first_half, shut[s], shut[s + 1]))
        bias = jnp.concatenate(bias, axis=1)
        keys = gathered[...]
        outs = []
        for d in range(n_dp):
            query_pair = queries[block, 2 * d : 2 * d + 2].reshape(pair_rows, 2 * HEAD_WIDTH)
            scores = lax.dot_general(
                query_pair, keys, (((1,), (1,)), ((), ())), preferred_element_type=jnp.float32
            )
            scores = scores + bias
            expon = jnp.exp(scores - jnp.max(scores, axis=1, keepdims=True))
            total = jnp.sum(expon, axis=1, keepdims=True)
            probs = (expon * (1.0 / total)).astype(jnp.bfloat16)
            mixed = jnp.dot(probs, keys, preferred_element_type=jnp.float32)
            even = pltpu.roll(mixed[:BLOCK_LENGTH], HEAD_WIDTH, 1)
            odd = mixed[BLOCK_LENGTH:]
            outs.append(
                jnp.where(first_half[:BLOCK_LENGTH], even, odd).astype(jnp.bfloat16)
            )
        rows = pl.ds(pl.multiple_of(block * BLOCK_LENGTH, BLOCK_LENGTH), BLOCK_LENGTH)
        attended[rows, :] = jnp.concatenate(outs, axis=1)
        return carry

    lax.fori_loop(0, blocks, attend, 0)

    out_right.wait_recv()
    out_on.wait_recv()

    rows_out = part_mine.shape[0]

    def project(which):
        rows = attended[pl.ds(pl.multiple_of(which * rows_out, rows_out), rows_out), :]
        return lax.dot_general(
            rows, out_all[...], (((1,), (1,)), ((), ())), preferred_element_type=jnp.float32
        )

    part_send[...] = project(1 - tp).astype(jnp.bfloat16)
    swap = remote(part_send, part_recv, half_sem.at[0], half_sem.at[1], dp, kv, 1 - tp)
    swap.start()
    part_mine[...] = project(tp)
    swap.wait_recv()
    mixed = part_mine[...] + part_recv[...].astype(jnp.float32)
    scale = lax.rsqrt(jnp.mean(mixed * mixed, axis=1, keepdims=True) + 1e-06)
    result_ref[...] = (mixed * scale * gain_ref[...]).astype(jnp.bfloat16)

    drain(others, pair_sem.at[0])
    drain(requests_all.at[pl.ds(0, n_kv - 1)], request_sem.at[0])
    drain(row_others, y_sem.at[0])
    drain(row_others, y_sem.at[2])
    for copy in (query_right, query_left, out_right, out_left, query_on, out_on):
        copy.wait_send()

    def drain_blocks(to, carry):
        @pl.when(to > kv)
        def _():
            block_copy(kv, to).wait_send()

        return carry

    lax.fori_loop(0, n_kv, drain_blocks, 0)
    swap.wait_send()


def index_tables(chosen, device, n_kv, blocks):
    safe = jnp.maximum(chosen, 0)
    targets = jnp.arange(n_kv * blocks, dtype=jnp.int32)
    hit = (chosen.reshape(-1, 1) == targets[None, :]).astype(jnp.int32)
    wanted = jnp.max(hit, axis=0)
    grid = wanted.reshape(n_kv, blocks)
    place = jnp.arange(blocks, dtype=jnp.int32)
    below = (place[:, None] > place[None, :]).astype(jnp.int32)
    rank = jnp.sum(grid[:, None, :] * below[None], axis=2)
    slots = [jnp.max(jnp.where((grid > 0) & (rank == s), place[None], 0), axis=1) for s in range(CAP)]
    requests = jnp.pad(jnp.stack(slots, axis=1), ((0, 0), (0, 128 - CAP)))[:, None, :]
    flat = safe.reshape(-1, 1)
    same = (flat // blocks == targets[None, :] // blocks) & (targets[None, :] < flat)
    slot = jnp.minimum(jnp.sum(jnp.where(same, wanted[None, :], 0), axis=1), CAP - 1)
    slot = slot.reshape(chosen.shape)
    owner = safe // blocks
    placed = jnp.where(owner == device, n_kv * CAP + safe - owner * blocks, owner * CAP + slot)
    return requests, jnp.where(chosen < 0, -1, placed)


def per_device(dims, tokens, chosen, query_weight, key_matrix, value_matrix, out_weight, out_gain):
    n_dp, n_kv, n_y = dims
    rows, width = tokens.shape
    blocks = rows // BLOCK_LENGTH
    heads_width = query_weight.shape[1]
    requests, placed = index_tables(chosen, lax.axis_index("kv"), n_kv, blocks)
    pair = jnp.concatenate([key_matrix, value_matrix], axis=1)
    pair_width = pair.shape[1]
    half_rows = rows // 2
    vmem, dma = pltpu.VMEM, pltpu.SemaphoreType.DMA
    bf16, f32, i32 = jnp.bfloat16, jnp.float32, jnp.int32
    in_vmem = pl.BlockSpec(memory_space=pltpu.VMEM)
    return pl.pallas_call(
        functools.partial(fused_kernel, dims),
        out_shape=jax.ShapeDtypeStruct((half_rows, width), bf16),
        in_specs=[
            pl.BlockSpec(memory_space=pltpu.SMEM),
            in_vmem,
            pl.BlockSpec(memory_space=pl.ANY),
            in_vmem,
            in_vmem,
            in_vmem,
            in_vmem,
        ],
        out_specs=in_vmem,
        scratch_shapes=[
            vmem((rows, width), bf16),
            vmem((width, pair_width), bf16),
            vmem((n_kv, 1, 128), i32),
            pltpu.SMEM((n_kv, 1, 128), i32),
            vmem((width, heads_width), bf16),
            vmem((width, heads_width), bf16),
            vmem((blocks, BLOCK_LENGTH, pair_width), bf16),
            vmem((n_kv * CAP + blocks, BLOCK_LENGTH, pair_width), bf16),
            vmem((n_kv, CAP, BLOCK_LENGTH, pair_width), bf16),
            vmem((blocks, heads_width // HEAD_WIDTH, BLOCK_LENGTH, pair_width), bf16),
            vmem((chosen.shape[1] * BLOCK_LENGTH, pair_width), bf16),
            vmem((rows, heads_width), bf16),
            vmem((half_rows, width), f32),
            vmem((half_rows, width), bf16),
            vmem((half_rows, width), bf16),
            dma,
            dma,
            dma((2,)),
            dma((2,)),
            dma((4,)),
            dma((16,)),
            dma((16,)),
            dma((6,)),
            dma((6,)),
            dma((n_kv,)),
            dma((n_kv,)),
            dma((2,)),
        ],
        compiler_params=pltpu.CompilerParams(
            collective_id=0, has_side_effects=True, vmem_limit_bytes=60 * 1024 * 1024
        ),
        name="fused",
    )(placed, requests, tokens, pair, query_weight, out_weight.T, out_gain[None, :])


def solution(mesh):
    n_dp, n_kv = mesh.shape["dp"], mesh.shape["kv"]
    n_y = 8
    placed = (
        P(("dp", "kv"), None),
        P(("dp", "kv"), None),
        P("kv", "tp"),
        P("kv", "tp"),
        P("kv", "tp"),
        P("tp", "kv"),
        P(),
    )
    return jax.shard_map(
        functools.partial(per_device, (n_dp, n_kv, n_y)),
        mesh=mesh,
        in_specs=placed,
        out_specs=P(("dp", "kv", "tp"), None),
        check_vma=False,
    )
```

```python
import functools

import jax
import jax.numpy as jnp
from jax import lax
from jax.experimental import pallas as pl
from jax.experimental.pallas import tpu as pltpu
from jax.sharding import PartitionSpec as P

HEAD_WIDTH = 64
BLOCK_LENGTH = 64
CAP = 2
NEAR = 5
NEG = -1e30
MESH = pl.DeviceIdType.MESH


def fused_kernel(
    dims,
    placed_ref,
    requests_ref,
    tokens_hbm,
    pair_ref,
    query_ref,
    out_ref,
    gain_ref,
    result_ref,
    tokens,
    pair_all,
    requests_all,
    requests_smem,
    query_all,
    out_all,
    own,
    chain1,
    chain2,
    chain3,
    chain4,
    pool,
    packed,
    far_packed,
    relayed,
    queries,
    gathered,
    attended,
    part_mine,
    part_send,
    part_recv,
    tok_sem,
    smem_sem,
    pair_sem,
    request_sem,
    y_sem,
    ring_send,
    ring_recv,
    x_send,
    x_recv,
    chain_send,
    chain_recv,
    block_send,
    block_recv,
    relay_send,
    relay_recv,
    onward_send,
    half_sem,
):
    n_dp, n_kv, n_y = dims
    n_z = n_kv // n_y
    dp, kv, tp = lax.axis_index("dp"), lax.axis_index("kv"), lax.axis_index("tp")
    z, y = kv // n_y, lax.rem(kv, n_y)
    depth = pair_ref.shape[0]
    blocks = own.shape[0]
    quarter = query_ref.shape[1] // n_dp
    chains = (own, chain1, chain2, chain3, chain4)
    near = len(chains)
    n_far = n_z - near

    def remote(src, dst, send, recv, to_dp, to_kv, to_tp):
        return pltpu.make_async_remote_copy(
            src_ref=src,
            dst_ref=dst,
            send_sem=send,
            recv_sem=recv,
            device_id=(to_dp, to_kv, to_tp),
            device_id_type=MESH,
        )

    def drain(ref, sem):
        pltpu.make_async_copy(ref, ref, sem).wait()

    load_tokens = pltpu.make_async_copy(tokens_hbm, tokens, tok_sem)
    load_tokens.start()

    barrier = pltpu.get_barrier_semaphore()

    def greet(off, carry):
        other = lax.rem(kv + off, n_kv)
        pl.semaphore_signal(barrier, inc=1, device_id=(dp, other, tp), device_id_type=MESH)
        return carry

    lax.fori_loop(1, n_kv, greet, 0)
    for off in range(1, n_dp):
        pl.semaphore_signal(
            barrier, inc=1, device_id=(lax.rem(dp + off, n_dp), kv, tp), device_id_type=MESH
        )
    pl.semaphore_signal(barrier, inc=1, device_id=(dp, kv, 1 - tp), device_id_type=MESH)

    my_rows = pl.ds(pl.multiple_of(kv * depth, depth), depth)
    my_cols = pl.ds(pl.multiple_of(dp * quarter, quarter), quarter)
    pair_all[my_rows, :] = pair_ref[...]
    query_all[my_rows, my_cols] = query_ref[:, my_cols]
    out_all[my_rows, my_cols] = out_ref[:, my_cols]

    pl.semaphore_wait(barrier, n_kv - 1 + n_dp - 1 + 1)

    def send_row(off, carry):
        other = z * n_y + lax.rem(y + off, n_y)
        for at, (src, dst) in enumerate(((query_ref, query_all), (out_ref, out_all))):
            remote(
                src.at[:, my_cols],
                dst.at[my_rows, my_cols],
                y_sem.at[2 * at],
                y_sem.at[2 * at + 1],
                dp,
                other,
                tp,
            ).start()
        return carry

    lax.fori_loop(1, n_y, send_row, 0)

    def send_pair(off, carry):
        other = lax.rem(kv + off, n_kv)
        remote(
            pair_ref, pair_all.at[my_rows, :], pair_sem.at[0], pair_sem.at[1], dp, other, tp
        ).start()
        return carry

    lax.fori_loop(1, n_kv, send_pair, 0)

    def ask(column, row, at):
        remote(
            requests_ref.at[pl.ds(column, 1)],
            requests_all.at[pl.ds(at, 1)],
            request_sem.at[0],
            request_sem.at[1],
            dp,
            row * n_y + column,
            tp,
        ).start()

    def ask_row(off, carry):
        ask(lax.rem(y + off, n_y), z, y)
        return carry

    def ask_far(column, carry):
        for far in range(n_far):
            ask(column, lax.rem(z + n_z - near - far, n_z), n_y * (1 + far) + y)
        return carry

    lax.fori_loop(1, n_y, ask_row, 0)
    lax.fori_loop(0, n_y, ask_far, 0)
    asked = requests_all.at[pl.ds(0, n_y * (1 + n_far) - 1)]

    others = pair_all.at[pl.ds(0, (n_kv - 1) * depth), :]
    row_others = pair_all.at[pl.ds(0, (n_y - 1) * depth), :]

    above = lax.rem(z + 1, n_z) * n_y + y
    below = lax.rem(z + n_z - 1, n_z) * n_y + y
    right, left = lax.rem(dp + 1, n_dp), lax.rem(dp + n_dp - 1, n_dp)
    bundle_depth = n_y * depth
    downs = 2
    ups = n_z - 1 - downs

    def bundle(ref, delta, which):
        start = pl.multiple_of(lax.rem(z + n_z + delta, n_z) * bundle_depth, bundle_depth)
        cols = pl.multiple_of(lax.rem(dp + n_dp + which, n_dp) * quarter, quarter)
        return ref.at[pl.ds(start, bundle_depth), pl.ds(cols, quarter)]

    def ring(step, up):
        copies = []
        for part, ref in enumerate((query_all, out_all)):
            piece = bundle(ref, 1 - step if up else step - 1, 0)
            at = 2 * (step - 1 if up else ups + step - 1) + part
            copies.append(
                remote(
                    piece, piece, ring_send.at[at], ring_recv.at[at], dp, above if up else below, tp
                )
            )
        return copies

    def across(delta, kind):
        ref = out_all if kind in (2, 3, 5) else query_all
        which = {4: -1, 5: 1}.get(kind, 0)
        piece = bundle(ref, delta, which)
        at = lax.rem(z + n_z + delta, n_z) * 6 + kind
        to = right if kind in (0, 2, 4) else left
        return remote(piece, piece, x_send.at[at], x_recv.at[at], to, kv, tp)

    def cross(delta):
        for kind in range(4):
            across(delta, kind).start()

    def cross_on(delta):
        across(delta, 0).wait_recv()
        across(delta, 4).start()
        across(delta, 3).wait_recv()
        across(delta, 5).start()

    def start(copies):
        for copy in copies:
            copy.start()

    def arrive(copies):
        for copy in copies:
            copy.wait_recv()

    drain(row_others, y_sem.at[1])
    drain(row_others, y_sem.at[3])
    start(ring(1, True))
    start(ring(1, False))
    cross(0)

    drain(asked, request_sem.at[1])
    to_smem = pltpu.make_async_copy(requests_all, requests_smem, smem_sem)
    to_smem.start()
    load_tokens.wait()
    drain(others, pair_sem.at[1])
    pairs = jnp.dot(tokens[...], pair_all[...], preferred_element_type=jnp.float32)
    pairs = pairs.astype(jnp.bfloat16).reshape(own.shape)
    own[...] = pairs
    pool[pl.ds(n_kv * CAP, blocks)] = pairs
    to_smem.wait()

    def climb(step):
        return remote(
            chains[step - 1],
            chains[step],
            chain_send.at[step - 1],
            chain_recv.at[step - 1],
            dp,
            above,
            tp,
        )

    def climb_on(step):
        @pl.when((z + 1 < n_z) & (z >= step - 1))
        def _():
            climb(step).start()

    def slots(owner):
        return pool.at[pl.ds(owner * CAP, CAP)]

    def far_copy(far, column):
        return remote(
            far_packed.at[far, column],
            relayed.at[far, y],
            relay_send.at[far * n_y + column],
            relay_recv.at[far * n_y + y],
            dp,
            z * n_y + column,
            tp,
        )

    def far_own(far):
        return remote(
            far_packed.at[far, y],
            slots(kv),
            relay_send.at[far * n_y + y],
            block_recv.at[kv],
            dp,
            (z + near + far) * n_y + y,
            tp,
        )

    def onward(far, column):
        owner = z * n_y + column
        return remote(
            relayed.at[far, column],
            slots(owner),
            onward_send.at[far * n_y + column],
            block_recv.at[owner],
            dp,
            (z + near + far) * n_y + y,
            tp,
        )

    def send_far(far):
        def one(off, carry):
            column = lax.rem(y + off, n_y)
            for slot in range(CAP):
                at = requests_smem[n_y * (1 + far) + column, 0, CAP * (near + far) + slot]
                far_packed[far, column, slot] = own[at]

            @pl.when(off > 0)
            def _():
                far_copy(far, column).start()

            @pl.when(off == 0)
            def _():
                far_own(far).start()

            return carry

        @pl.when(z + near + far < n_z)
        def _():
            lax.fori_loop(0, n_y, one, 0)

    def pass_far(far):
        def one(off, carry):
            column = lax.rem(y + off, n_y)
            relay = remote(
                far_packed.at[far, y],
                relayed.at[far, column],
                relay_send.at[far * n_y + y],
                relay_recv.at[far * n_y + column],
                dp,
                kv,
                tp,
            )
            relay.wait_recv()
            onward(far, column).start()
            return carry

        @pl.when(z + near + far < n_z)
        def _():
            lax.fori_loop(1, n_y, one, 0)

    def near_copy(step, column):
        owner = (z - step) * n_y + y
        return remote(
            packed.at[step, column],
            slots(owner),
            block_send.at[step * n_y + column],
            block_recv.at[owner],
            dp,
            z * n_y + column,
            tp,
        )

    def share(step):
        def one(off, carry):
            column = lax.rem(y + off, n_y)

            @pl.when((column > y) | (step > 0))
            def _():
                for slot in range(CAP):
                    at = requests_smem[column, 0, CAP * step + slot]
                    packed[step, column, slot] = chains[step][at]
                near_copy(step, column).start()

            return carry

        lax.fori_loop(1, n_y, one, 0)

    def take_chain(step):
        @pl.when(z >= step)
        def _():
            climb(step).wait_recv()

        if step + 1 < near:
            climb_on(step + 1)

        @pl.when(z >= step)
        def _():
            pool[pl.ds(n_kv * CAP + step * blocks, blocks)] = chains[step][...]
            share(step)

    climb_on(1)
    for far in reversed(range(n_far)):
        send_far(far)
    share(0)

    arrive(ring(1, True))
    arrive(ring(1, False))
    start(ring(2, True))
    start(ring(2, False))
    cross(-1)
    cross(1)

    pass_far(2)
    take_chain(1)
    cross_on(0)

    arrive(ring(2, True))
    arrive(ring(2, False))
    start(ring(3, True))
    cross(-2)
    cross(2)

    pass_far(1)
    take_chain(2)
    cross_on(-1)
    cross_on(1)

    arrive(ring(3, True))
    start(ring(4, True))
    cross(-3)

    pass_far(0)
    take_chain(3)
    cross_on(-2)
    cross_on(2)

    arrive(ring(4, True))
    start(ring(5, True))
    cross(-4)

    take_chain(4)
    cross_on(-3)
    arrive(ring(5, True))
    cross(-5)
    cross_on(-4)
    cross_on(-5)

    def wait_across(kinds):
        def one(at, carry):
            for kind in kinds:
                across(at - z, kind).wait_recv()
            return carry

        lax.fori_loop(0, n_z, one, 0)

    wait_across((1, 4))

    lane = lax.broadcasted_iota(jnp.int32, (tokens.shape[0], 2 * HEAD_WIDTH), 1)
    for d in range(n_dp):
        rows = jnp.dot(
            tokens[...],
            query_all[:, d * quarter : (d + 1) * quarter],
            preferred_element_type=jnp.float32,
        )
        rows = rows.astype(jnp.bfloat16).astype(jnp.float32) * HEAD_WIDTH ** (-0.5)
        turned = pltpu.roll(rows, HEAD_WIDTH, 1)
        for side, value in enumerate((rows, turned)):
            head = jnp.where(lane < HEAD_WIDTH, value, 0.0).astype(jnp.bfloat16)
            queries[:, 2 * d + side] = head.reshape(blocks, BLOCK_LENGTH, 2 * HEAD_WIDTH)

    def wait_blocks(owner, carry):
        steps = z - owner // n_y
        mate = lax.rem(owner, n_y)
        expected = (owner < kv) & ((steps == 0) | (steps >= near) | (mate != y))

        @pl.when(expected)
        def _():
            remote(
                packed.at[0, 0], slots(owner), block_send.at[0], block_recv.at[owner], dp, kv, tp
            ).wait_recv()

        return carry

    lax.fori_loop(0, n_kv, wait_blocks, 0)

    sel = placed_ref.shape[1]
    pair_rows = 2 * BLOCK_LENGTH
    row_at = lax.broadcasted_iota(jnp.int32, (pair_rows, 2 * HEAD_WIDTH), 0)
    lane_at = lax.broadcasted_iota(jnp.int32, (pair_rows, 2 * HEAD_WIDTH), 1)
    first_half = lane_at < BLOCK_LENGTH
    own_bias = jnp.where(lane_at <= lax.rem(row_at, BLOCK_LENGTH), 0.0, NEG)

    def attend(block, carry):
        shut = []
        for s in range(sel):
            at = placed_ref[block, s]
            gathered[s * BLOCK_LENGTH : (s + 1) * BLOCK_LENGTH, :] = pool[jnp.maximum(at, 0)]
            shut.append(jnp.where(at < 0, NEG, 0.0))
        bias = [jnp.where(first_half, own_bias, shut[1])]
        for s in range(2, sel, 2):
            bias.append(jnp.where(first_half, shut[s], shut[s + 1]))
        bias = jnp.concatenate(bias, axis=1)
        keys = gathered[...]
        outs = []
        for d in range(n_dp):
            query_pair = queries[block, 2 * d : 2 * d + 2].reshape(pair_rows, 2 * HEAD_WIDTH)
            scores = lax.dot_general(
                query_pair, keys, (((1,), (1,)), ((), ())), preferred_element_type=jnp.float32
            )
            scores = scores + bias
            expon = jnp.exp(scores - jnp.max(scores, axis=1, keepdims=True))
            total = jnp.sum(expon, axis=1, keepdims=True)
            probs = (expon * (1.0 / total)).astype(jnp.bfloat16)
            mixed = jnp.dot(probs, keys, preferred_element_type=jnp.float32)
            even = pltpu.roll(mixed[:BLOCK_LENGTH], HEAD_WIDTH, 1)
            odd = mixed[BLOCK_LENGTH:]
            outs.append(
                jnp.where(first_half[:BLOCK_LENGTH], even, odd).astype(jnp.bfloat16)
            )
        rows = pl.ds(pl.multiple_of(block * BLOCK_LENGTH, BLOCK_LENGTH), BLOCK_LENGTH)
        attended[rows, :] = jnp.concatenate(outs, axis=1)
        return carry

    lax.fori_loop(0, blocks, attend, 0)

    wait_across((2, 5))

    rows_out = part_mine.shape[0]

    def project(which):
        rows = attended[pl.ds(pl.multiple_of(which * rows_out, rows_out), rows_out), :]
        return lax.dot_general(
            rows, out_all[...], (((1,), (1,)), ((), ())), preferred_element_type=jnp.float32
        )

    part_send[...] = project(1 - tp).astype(jnp.bfloat16)
    swap = remote(part_send, part_recv, half_sem.at[0], half_sem.at[1], dp, kv, 1 - tp)
    swap.start()
    part_mine[...] = project(tp)
    swap.wait_recv()
    mixed = part_mine[...] + part_recv[...].astype(jnp.float32)
    scale = lax.rsqrt(jnp.mean(mixed * mixed, axis=1, keepdims=True) + 1e-06)
    result_ref[...] = (mixed * scale * gain_ref[...]).astype(jnp.bfloat16)

    drain(others, pair_sem.at[0])
    drain(asked, request_sem.at[0])
    drain(row_others, y_sem.at[0])
    drain(row_others, y_sem.at[2])
    for step in range(1, ups + 1):
        for copy in ring(step, True):
            copy.wait_send()
    for step in range(1, downs + 1):
        for copy in ring(step, False):
            copy.wait_send()

    def drain_across(at, carry):
        for kind in range(6):
            across(at - z, kind).wait_send()
        return carry

    lax.fori_loop(0, n_z, drain_across, 0)

    for step in range(near):
        if step + 1 < near:

            @pl.when((z + 1 < n_z) & (z >= step))
            def _(step=step):
                climb(step + 1).wait_send()

        def drain_near(off, carry, step=step):
            column = lax.rem(y + off, n_y)

            @pl.when((z >= step) & ((column > y) | (step > 0)))
            def _():
                near_copy(step, column).wait_send()

            return carry

        lax.fori_loop(1, n_y, drain_near, 0)

    for far in range(n_far):

        def drain_far(off, carry, far=far):
            column = lax.rem(y + off, n_y)
            far_copy(far, column).wait_send()

            @pl.when(off > 0)
            def _():
                onward(far, column).wait_send()

            return carry

        @pl.when(z + near + far < n_z)
        def _(drain_far=drain_far):
            lax.fori_loop(0, n_y, drain_far, 0)

    swap.wait_send()


def index_tables(chosen, device, n_kv, n_y, blocks):
    n_z = n_kv // n_y
    z, y = device // n_y, device % n_y
    safe = jnp.maximum(chosen, 0)
    targets = jnp.arange(n_kv * blocks, dtype=jnp.int32)
    hit = (chosen.reshape(-1, 1) == targets[None, :]).astype(jnp.int32)
    wanted = jnp.max(hit, axis=0)
    grid = wanted.reshape(n_kv, blocks)
    place = jnp.arange(blocks, dtype=jnp.int32)
    below = (place[:, None] > place[None, :]).astype(jnp.int32)
    rank = jnp.sum(grid[:, None, :] * below[None], axis=2)
    slots = [jnp.max(jnp.where((grid > 0) & (rank == s), place[None], 0), axis=1) for s in range(CAP)]
    table = jnp.stack(slots, axis=1).reshape(n_z, n_y, CAP)
    table = jnp.take(table, (z - jnp.arange(n_z)) % n_z, axis=0)
    table = table.transpose(1, 0, 2).reshape(n_y, n_z * CAP)
    requests = jnp.pad(table, ((0, 0), (0, 128 - n_z * CAP)))[:, None, :]
    flat = safe.reshape(-1, 1)
    same = (flat // blocks == targets[None, :] // blocks) & (targets[None, :] < flat)
    slot = jnp.minimum(jnp.sum(jnp.where(same, wanted[None, :], 0), axis=1), CAP - 1)
    slot = slot.reshape(chosen.shape)
    owner = safe // blocks
    steps = z - owner // n_y
    whole = (owner % n_y == y) & (steps >= 0) & (steps < NEAR)
    inside = n_kv * CAP + steps * blocks + safe - owner * blocks
    placed = jnp.where(whole, inside, owner * CAP + slot)
    return requests, jnp.where(chosen < 0, -1, placed)


def per_device(dims, tokens, chosen, query_weight, key_matrix, value_matrix, out_weight, out_gain):
    n_dp, n_kv, n_y = dims
    rows, width = tokens.shape
    blocks = rows // BLOCK_LENGTH
    heads_width = query_weight.shape[1]
    requests, placed = index_tables(chosen, lax.axis_index("kv"), n_kv, n_y, blocks)
    pair = jnp.concatenate([key_matrix, value_matrix], axis=1)
    pair_width = pair.shape[1]
    half_rows = rows // 2
    n_z = n_kv // n_y
    far = n_z - NEAR
    vmem, dma = pltpu.VMEM, pltpu.SemaphoreType.DMA
    bf16, f32, i32 = jnp.bfloat16, jnp.float32, jnp.int32
    in_vmem = pl.BlockSpec(memory_space=pltpu.VMEM)
    return pl.pallas_call(
        functools.partial(fused_kernel, dims),
        out_shape=jax.ShapeDtypeStruct((half_rows, width), bf16),
        in_specs=[
            pl.BlockSpec(memory_space=pltpu.SMEM),
            in_vmem,
            pl.BlockSpec(memory_space=pl.ANY),
            in_vmem,
            in_vmem,
            in_vmem,
            in_vmem,
        ],
        out_specs=in_vmem,
        scratch_shapes=[
            vmem((rows, width), bf16),
            vmem((width, pair_width), bf16),
            vmem((n_y * (1 + far), 1, 128), i32),
            pltpu.SMEM((n_y * (1 + far), 1, 128), i32),
            vmem((width, heads_width), bf16),
            vmem((width, heads_width), bf16),
            *[vmem((blocks, BLOCK_LENGTH, pair_width), bf16)] * NEAR,
            vmem((n_kv * CAP + NEAR * blocks, BLOCK_LENGTH, pair_width), bf16),
            vmem((NEAR, n_y, CAP, BLOCK_LENGTH, pair_width), bf16),
            vmem((far, n_y, CAP, BLOCK_LENGTH, pair_width), bf16),
            vmem((far, n_y, CAP, BLOCK_LENGTH, pair_width), bf16),
            vmem((blocks, heads_width // HEAD_WIDTH, BLOCK_LENGTH, pair_width), bf16),
            vmem((chosen.shape[1] * BLOCK_LENGTH, pair_width), bf16),
            vmem((rows, heads_width), bf16),
            vmem((half_rows, width), f32),
            vmem((half_rows, width), bf16),
            vmem((half_rows, width), bf16),
            dma,
            dma,
            dma((2,)),
            dma((2,)),
            dma((4,)),
            dma((2 * (n_z - 1),)),
            dma((2 * (n_z - 1),)),
            dma((6 * n_z,)),
            dma((6 * n_z,)),
            dma((NEAR - 1,)),
            dma((NEAR - 1,)),
            dma((NEAR * n_y,)),
            dma((n_kv,)),
            dma((far * n_y,)),
            dma((far * n_y,)),
            dma((far * n_y,)),
            dma((2,)),
        ],
        compiler_params=pltpu.CompilerParams(
            collective_id=0, has_side_effects=True, vmem_limit_bytes=60 * 1024 * 1024
        ),
        name="fused",
    )(placed, requests, tokens, pair, query_weight, out_weight.T, out_gain[None, :])


def solution(mesh):
    n_dp, n_kv = mesh.shape["dp"], mesh.shape["kv"]
    n_y = 8
    placed = (
        P(("dp", "kv"), None),
        P(("dp", "kv"), None),
        P("kv", "tp"),
        P("kv", "tp"),
        P("kv", "tp"),
        P("tp", "kv"),
        P(),
    )
    return jax.shard_map(
        functools.partial(per_device, (n_dp, n_kv, n_y)),
        mesh=mesh,
        in_specs=placed,
        out_specs=P(("dp", "kv", "tp"), None),
        check_vma=False,
    )
```

```python
import functools

import jax
import jax.numpy as jnp
from jax import lax
from jax.experimental import pallas as pl
from jax.experimental.pallas import tpu as pltpu
from jax.sharding import PartitionSpec as P

HEAD_WIDTH = 64
BLOCK_LENGTH = 64
CAP = 2
NEAR = 5
NEG = -1e30
MESH = pl.DeviceIdType.MESH


def fused_kernel(
    dims,
    chosen_ref,
    chosen_rows,
    tokens_hbm,
    key_ref,
    value_ref,
    query_ref,
    out_ref,
    result_ref,
    placed_vmem,
    placed_ref,
    requests_ref,
    tokens,
    pair_all,
    requests_all,
    requests_smem,
    query_all,
    out_all,
    own,
    chain1,
    chain2,
    chain3,
    chain4,
    pool,
    packed,
    far_packed,
    relayed,
    queries,
    gathered,
    attended,
    part_mine,
    part_send,
    part_recv,
    tok_sem,
    place_sem,
    smem_sem,
    pair_sem,
    request_sem,
    y_sem,
    ring_send,
    ring_recv,
    x_send,
    x_recv,
    chain_send,
    chain_recv,
    block_send,
    block_recv,
    relay_send,
    relay_recv,
    onward_send,
    half_sem,
):
    n_dp, n_kv, n_y = dims
    n_z = n_kv // n_y
    dp, kv, tp = lax.axis_index("dp"), lax.axis_index("kv"), lax.axis_index("tp")
    z, y = kv // n_y, lax.rem(kv, n_y)
    depth = key_ref.shape[0]
    blocks = own.shape[0]
    quarter = query_ref.shape[1] // n_dp
    chains = (own, chain1, chain2, chain3, chain4)
    near = len(chains)
    n_far = n_z - near

    def remote(src, dst, send, recv, to_dp, to_kv, to_tp):
        return pltpu.make_async_remote_copy(
            src_ref=src,
            dst_ref=dst,
            send_sem=send,
            recv_sem=recv,
            device_id=(to_dp, to_kv, to_tp),
            device_id_type=MESH,
        )

    def drain(ref, sem):
        pltpu.make_async_copy(ref, ref, sem).wait()

    load_tokens = pltpu.make_async_copy(tokens_hbm, tokens, tok_sem)
    load_tokens.start()

    barrier = pltpu.get_barrier_semaphore()

    def greet(off, carry):
        other = lax.rem(kv + off, n_kv)
        pl.semaphore_signal(barrier, inc=1, device_id=(dp, other, tp), device_id_type=MESH)
        return carry

    lax.fori_loop(1, n_kv, greet, 0)
    for off in range(1, n_dp):
        pl.semaphore_signal(
            barrier, inc=1, device_id=(lax.rem(dp + off, n_dp), kv, tp), device_id_type=MESH
        )
    pl.semaphore_signal(barrier, inc=1, device_id=(dp, kv, 1 - tp), device_id_type=MESH)

    my_rows = pl.ds(pl.multiple_of(kv * depth, depth), depth)
    my_cols = pl.ds(pl.multiple_of(dp * quarter, quarter), quarter)
    wide = jnp.float32
    pair = jnp.concatenate([key_ref[...].astype(wide), value_ref[...].astype(wide)], axis=1)
    pair_all[my_rows, :] = pair.astype(jnp.bfloat16)
    query_all[my_rows, my_cols] = query_ref[:, my_cols]
    out_all[my_rows, my_cols] = out_ref[:, my_cols]

    sel = chosen_ref.shape[1]
    table_lane = lax.broadcasted_iota(jnp.int32, (n_y, 128), 1)
    table_owner = lax.rem(z + n_z - lax.rem(table_lane // CAP, n_z), n_z) * n_y
    table_owner = table_owner + lax.broadcasted_iota(jnp.int32, (n_y, 128), 0)
    table_last = lax.rem(table_lane, CAP) > 0
    rows_at = chosen_rows[...]
    rows_owner = jnp.right_shift(rows_at, 3)

    def tabulate(at, carry):
        first, last, later = carry
        for s in range(sel):
            block = chosen_ref[at, s]
            owner = jnp.right_shift(block, 3)
            inner = jnp.bitwise_and(block, blocks - 1)
            mine = table_owner == owner
            first = jnp.where(mine, jnp.minimum(first, inner), first)
            last = jnp.where(mine, jnp.maximum(last, inner), last)
            later = jnp.where((rows_owner == owner) & (rows_at > block), 1, later)
        return first, last, later

    zeros = jnp.zeros((n_y, 128), jnp.int32)
    first, last, later = lax.fori_loop(
        0, blocks, tabulate, (zeros + (blocks - 1), zeros, jnp.zeros(rows_at.shape, jnp.int32))
    )
    requests_ref[...] = jnp.where(table_last, last, first).reshape(requests_ref.shape)
    steps_up = z - jnp.right_shift(rows_owner, 3)
    whole = (jnp.bitwise_and(rows_owner, n_y - 1) == y) & (steps_up < near)
    inside = n_kv * CAP + steps_up * blocks + jnp.bitwise_and(rows_at, blocks - 1)
    placed = jnp.where(whole, inside, rows_owner * CAP + later)
    placed_vmem[...] = jnp.zeros_like(placed_vmem)
    placed_vmem[:, :sel] = jnp.where(rows_at < 0, -1, placed)
    to_placed = pltpu.make_async_copy(placed_vmem, placed_ref, place_sem)
    to_placed.start()

    pl.semaphore_wait(barrier, n_kv - 1 + n_dp - 1 + 1)

    def send_row(off, carry):
        other = z * n_y + lax.rem(y + off, n_y)
        for at, dst in enumerate((query_all, out_all)):
            remote(
                dst.at[my_rows, my_cols],
                dst.at[my_rows, my_cols],
                y_sem.at[2 * at],
                y_sem.at[2 * at + 1],
                dp,
                other,
                tp,
            ).start()
        return carry

    lax.fori_loop(1, n_y, send_row, 0)

    def send_pair(off, carry):
        other = lax.rem(kv + off, n_kv)
        mine = pair_all.at[my_rows, :]
        remote(mine, mine, pair_sem.at[0], pair_sem.at[1], dp, other, tp).start()
        return carry

    lax.fori_loop(1, n_kv, send_pair, 0)

    def ask(column, row, at):
        remote(
            requests_ref.at[pl.ds(column, 1)],
            requests_all.at[pl.ds(at, 1)],
            request_sem.at[0],
            request_sem.at[1],
            dp,
            row * n_y + column,
            tp,
        ).start()

    def ask_row(off, carry):
        ask(lax.rem(y + off, n_y), z, y)
        return carry

    def ask_far(column, carry):
        for far in range(n_far):
            ask(column, lax.rem(z + n_z - near - far, n_z), n_y * (1 + far) + y)
        return carry

    lax.fori_loop(1, n_y, ask_row, 0)
    lax.fori_loop(0, n_y, ask_far, 0)
    asked = requests_all.at[pl.ds(0, n_y * (1 + n_far) - 1)]

    others = pair_all.at[pl.ds(0, (n_kv - 1) * depth), :]
    row_others = pair_all.at[pl.ds(0, (n_y - 1) * depth), :]

    above = lax.rem(z + 1, n_z) * n_y + y
    below = lax.rem(z + n_z - 1, n_z) * n_y + y
    right, left = lax.rem(dp + 1, n_dp), lax.rem(dp + n_dp - 1, n_dp)
    bundle_depth = n_y * depth
    downs = 2
    ups = n_z - 1 - downs

    def bundle(ref, delta, which):
        start = pl.multiple_of(lax.rem(z + n_z + delta, n_z) * bundle_depth, bundle_depth)
        cols = pl.multiple_of(lax.rem(dp + n_dp + which, n_dp) * quarter, quarter)
        return ref.at[pl.ds(start, bundle_depth), pl.ds(cols, quarter)]

    def ring(step, up):
        copies = []
        for part, ref in enumerate((query_all, out_all)):
            piece = bundle(ref, 1 - step if up else step - 1, 0)
            at = 2 * (step - 1 if up else ups + step - 1) + part
            copies.append(
                remote(
                    piece, piece, ring_send.at[at], ring_recv.at[at], dp, above if up else below, tp
                )
            )
        return copies

    def across(delta, kind):
        ref = out_all if kind in (2, 3, 5) else query_all
        which = {4: -1, 5: 1}.get(kind, 0)
        piece = bundle(ref, delta, which)
        at = lax.rem(z + n_z + delta, n_z) * 6 + kind
        to = right if kind in (0, 2, 4) else left
        return remote(piece, piece, x_send.at[at], x_recv.at[at], to, kv, tp)

    def cross(delta):
        for kind in range(4):
            across(delta, kind).start()

    def cross_on(delta):
        across(delta, 0).wait_recv()
        across(delta, 4).start()
        across(delta, 3).wait_recv()
        across(delta, 5).start()

    def start(copies):
        for copy in copies:
            copy.start()

    def arrive(copies):
        for copy in copies:
            copy.wait_recv()

    drain(row_others, y_sem.at[1])
    drain(row_others, y_sem.at[3])
    start(ring(1, True))
    start(ring(1, False))
    cross(0)
    arrive(ring(1, True))
    arrive(ring(1, False))
    start(ring(2, True))
    start(ring(2, False))
    cross(-1)
    cross(1)

    drain(asked, request_sem.at[1])
    to_smem = pltpu.make_async_copy(requests_all, requests_smem, smem_sem)
    to_smem.start()
    load_tokens.wait()
    drain(others, pair_sem.at[1])
    pairs = jnp.dot(tokens[...], pair_all[...], preferred_element_type=jnp.float32)
    pairs = pairs.astype(jnp.bfloat16).reshape(own.shape)
    own[...] = pairs
    pool[pl.ds(n_kv * CAP, blocks)] = pairs
    to_smem.wait()

    def climb(step):
        return remote(
            chains[step - 1],
            chains[step],
            chain_send.at[step - 1],
            chain_recv.at[step - 1],
            dp,
            above,
            tp,
        )

    def climb_on(step):
        @pl.when((z + 1 < n_z) & (z >= step - 1))
        def _():
            climb(step).start()

    def slots(owner):
        return pool.at[pl.ds(owner * CAP, CAP)]

    def far_copy(far, column):
        return remote(
            far_packed.at[far, column],
            relayed.at[far, y],
            relay_send.at[far * n_y + column],
            relay_recv.at[far * n_y + y],
            dp,
            z * n_y + column,
            tp,
        )

    def far_own(far):
        return remote(
            far_packed.at[far, y],
            slots(kv),
            relay_send.at[far * n_y + y],
            block_recv.at[kv],
            dp,
            (z + near + far) * n_y + y,
            tp,
        )

    def onward(far, column):
        owner = z * n_y + column
        return remote(
            relayed.at[far, column],
            slots(owner),
            onward_send.at[far * n_y + column],
            block_recv.at[owner],
            dp,
            (z + near + far) * n_y + y,
            tp,
        )

    def send_far(far):
        def one(off, carry):
            column = lax.rem(y + off, n_y)
            for slot in range(CAP):
                at = requests_smem[n_y * (1 + far) + column, 0, CAP * (near + far) + slot]
                far_packed[far, column, slot] = own[at]

            @pl.when(off > 0)
            def _():
                far_copy(far, column).start()

            @pl.when(off == 0)
            def _():
                far_own(far).start()

            return carry

        @pl.when(z + near + far < n_z)
        def _():
            lax.fori_loop(0, n_y, one, 0)

    def pass_far(far):
        def one(off, carry):
            column = lax.rem(y + off, n_y)
            relay = remote(
                far_packed.at[far, y],
                relayed.at[far, column],
                relay_send.at[far * n_y + y],
                relay_recv.at[far * n_y + column],
                dp,
                kv,
                tp,
            )
            relay.wait_recv()
            onward(far, column).start()
            return carry

        @pl.when(z + near + far < n_z)
        def _():
            lax.fori_loop(1, n_y, one, 0)

    def near_copy(step, column):
        owner = (z - step) * n_y + y
        return remote(
            packed.at[step, column],
            slots(owner),
            block_send.at[step * n_y + column],
            block_recv.at[owner],
            dp,
            z * n_y + column,
            tp,
        )

    def share(step):
        def one(off, carry):
            column = lax.rem(y + off, n_y)

            @pl.when((column > y) | (step > 0))
            def _():
                for slot in range(CAP):
                    at = requests_smem[column, 0, CAP * step + slot]
                    packed[step, column, slot] = chains[step][at]
                near_copy(step, column).start()

            return carry

        lax.fori_loop(1, n_y, one, 0)

    def take_chain(step):
        @pl.when(z >= step)
        def _():
            climb(step).wait_recv()

        if step + 1 < near:
            climb_on(step + 1)

        @pl.when(z >= step)
        def _():
            pool[pl.ds(n_kv * CAP + step * blocks, blocks)] = chains[step][...]
            share(step)

    climb_on(1)
    for far in reversed(range(n_far)):
        send_far(far)
    share(0)
    cross_on(0)

    arrive(ring(2, True))
    arrive(ring(2, False))
    start(ring(3, True))
    cross(-2)
    cross(2)
    pass_far(2)
    take_chain(1)
    cross_on(-1)
    cross_on(1)

    arrive(ring(3, True))
    start(ring(4, True))
    cross(-3)
    pass_far(1)
    take_chain(2)
    cross_on(-2)

    arrive(ring(4, True))
    start(ring(5, True))
    cross(-4)
    pass_far(0)
    take_chain(3)
    cross_on(2)
    cross_on(-3)

    arrive(ring(5, True))
    cross(-5)
    take_chain(4)
    cross_on(-4)
    cross_on(-5)

    def wait_across(kinds):
        def one(at, carry):
            for kind in kinds:
                across(at - z, kind).wait_recv()
            return carry

        lax.fori_loop(0, n_z, one, 0)

    wait_across((1, 4))

    lane = lax.broadcasted_iota(jnp.int32, (tokens.shape[0], 2 * HEAD_WIDTH), 1)
    for d in range(n_dp):
        rows = jnp.dot(
            tokens[...],
            query_all[:, d * quarter : (d + 1) * quarter],
            preferred_element_type=jnp.float32,
        )
        rows = rows.astype(jnp.bfloat16).astype(jnp.float32) * HEAD_WIDTH ** (-0.5)
        turned = pltpu.roll(rows, HEAD_WIDTH, 1)
        for side, value in enumerate((rows, turned)):
            head = jnp.where(lane < HEAD_WIDTH, value, 0.0).astype(jnp.bfloat16)
            queries[:, 2 * d + side] = head.reshape(blocks, BLOCK_LENGTH, 2 * HEAD_WIDTH)

    drain(others, pair_sem.at[0])
    drain(asked, request_sem.at[0])
    drain(row_others, y_sem.at[0])
    drain(row_others, y_sem.at[2])
    for step in range(1, ups + 1):
        for copy in ring(step, True):
            copy.wait_send()
    for step in range(1, downs + 1):
        for copy in ring(step, False):
            copy.wait_send()

    for step in range(near):
        if step + 1 < near:

            @pl.when((z + 1 < n_z) & (z >= step))
            def _(step=step):
                climb(step + 1).wait_send()

        def drain_near(off, carry, step=step):
            column = lax.rem(y + off, n_y)

            @pl.when((z >= step) & ((column > y) | (step > 0)))
            def _():
                near_copy(step, column).wait_send()

            return carry

        lax.fori_loop(1, n_y, drain_near, 0)

    for far in range(n_far):

        def drain_far(off, carry, far=far):
            column = lax.rem(y + off, n_y)
            far_copy(far, column).wait_send()

            @pl.when(off > 0)
            def _():
                onward(far, column).wait_send()

            return carry

        @pl.when(z + near + far < n_z)
        def _(drain_far=drain_far):
            lax.fori_loop(0, n_y, drain_far, 0)

    def wait_blocks(owner, carry):
        steps = z - owner // n_y
        mate = lax.rem(owner, n_y)
        expected = (owner < kv) & ((steps == 0) | (steps >= near) | (mate != y))

        @pl.when(expected)
        def _():
            remote(
                packed.at[0, 0], slots(owner), block_send.at[0], block_recv.at[owner], dp, kv, tp
            ).wait_recv()

        return carry

    lax.fori_loop(0, n_kv, wait_blocks, 0)
    to_placed.wait()

    pair_rows = 2 * BLOCK_LENGTH
    row_at = lax.broadcasted_iota(jnp.int32, (pair_rows, 2 * HEAD_WIDTH), 0)
    lane_at = lax.broadcasted_iota(jnp.int32, (pair_rows, 2 * HEAD_WIDTH), 1)
    first_half = lane_at < BLOCK_LENGTH
    own_bias = jnp.where(lane_at <= lax.rem(row_at, BLOCK_LENGTH), 0.0, NEG)

    def attend(block, carry):
        shut = []
        for s in range(sel):
            at = placed_ref[block, s]
            gathered[s * BLOCK_LENGTH : (s + 1) * BLOCK_LENGTH, :] = pool[jnp.maximum(at, 0)]
            shut.append(jnp.where(at < 0, NEG, 0.0))
        bias = [jnp.where(first_half, own_bias, shut[1])]
        for s in range(2, sel, 2):
            bias.append(jnp.where(first_half, shut[s], shut[s + 1]))
        bias = jnp.concatenate(bias, axis=1)
        keys = gathered[...]
        outs = []
        for d in range(n_dp):
            query_pair = queries[block, 2 * d : 2 * d + 2].reshape(pair_rows, 2 * HEAD_WIDTH)
            scores = lax.dot_general(
                query_pair, keys, (((1,), (1,)), ((), ())), preferred_element_type=jnp.float32
            )
            scores = scores + bias
            expon = jnp.exp(scores - jnp.max(scores, axis=1, keepdims=True))
            total = jnp.sum(expon, axis=1, keepdims=True)
            probs = expon.astype(jnp.bfloat16)
            mixed = jnp.dot(probs, keys, preferred_element_type=jnp.float32) * (1.0 / total)
            even = pltpu.roll(mixed[:BLOCK_LENGTH], HEAD_WIDTH, 1)
            odd = mixed[BLOCK_LENGTH:]
            outs.append(
                jnp.where(first_half[:BLOCK_LENGTH], even, odd).astype(jnp.bfloat16)
            )
        rows = pl.ds(pl.multiple_of(block * BLOCK_LENGTH, BLOCK_LENGTH), BLOCK_LENGTH)
        attended[rows, :] = jnp.concatenate(outs, axis=1)
        return carry

    lax.fori_loop(0, blocks, attend, 0)

    wait_across((2, 5))

    def drain_across(at, carry):
        for kind in range(6):
            across(at - z, kind).wait_send()
        return carry

    lax.fori_loop(0, n_z, drain_across, 0)

    rows_out = part_mine.shape[0]

    def project(which):
        rows = attended[pl.ds(pl.multiple_of(which * rows_out, rows_out), rows_out), :]
        return lax.dot_general(
            rows, out_all[...], (((1,), (1,)), ((), ())), preferred_element_type=jnp.float32
        )

    part_send[...] = project(1 - tp).astype(jnp.bfloat16)
    swap = remote(part_send, part_recv, half_sem.at[0], half_sem.at[1], dp, kv, 1 - tp)
    swap.start()
    part_mine[...] = project(tp)
    swap.wait_recv()
    mixed = part_mine[...] + part_recv[...].astype(jnp.float32)
    scale = lax.rsqrt(jnp.mean(mixed * mixed, axis=1, keepdims=True) + 1e-06)
    result_ref[...] = mixed * scale

    swap.wait_send()


def per_device(dims, tokens, chosen, query_weight, key_matrix, value_matrix, out_weight, out_gain):
    n_dp, n_kv, n_y = dims
    rows, width = tokens.shape
    blocks = rows // BLOCK_LENGTH
    heads_width = query_weight.shape[1]
    pair_width = key_matrix.shape[1] + value_matrix.shape[1]
    half_rows = rows // 2
    n_z = n_kv // n_y
    far = n_z - NEAR
    vmem, dma = pltpu.VMEM, pltpu.SemaphoreType.DMA
    bf16, f32, i32 = jnp.bfloat16, jnp.float32, jnp.int32
    in_vmem = pl.BlockSpec(memory_space=pltpu.VMEM)
    normed = pl.pallas_call(
        functools.partial(fused_kernel, dims),
        out_shape=jax.ShapeDtypeStruct((half_rows, width), f32),
        in_specs=[
            pl.BlockSpec(memory_space=pltpu.SMEM),
            in_vmem,
            pl.BlockSpec(memory_space=pl.ANY),
            in_vmem,
            in_vmem,
            in_vmem,
            in_vmem,
        ],
        out_specs=in_vmem,
        scratch_shapes=[
            vmem((blocks, 128), i32),
            pltpu.SMEM((blocks, 128), i32),
            vmem((n_y, 1, 128), i32),
            vmem((rows, width), bf16),
            vmem((width, pair_width), bf16),
            vmem((n_y * (1 + far), 1, 128), i32),
            pltpu.SMEM((n_y * (1 + far), 1, 128), i32),
            vmem((width, heads_width), bf16),
            vmem((width, heads_width), bf16),
            *[vmem((blocks, BLOCK_LENGTH, pair_width), bf16)] * NEAR,
            vmem((n_kv * CAP + NEAR * blocks, BLOCK_LENGTH, pair_width), bf16),
            vmem((NEAR, n_y, CAP, BLOCK_LENGTH, pair_width), bf16),
            vmem((far, n_y, CAP, BLOCK_LENGTH, pair_width), bf16),
            vmem((far, n_y, CAP, BLOCK_LENGTH, pair_width), bf16),
            vmem((blocks, heads_width // HEAD_WIDTH, BLOCK_LENGTH, pair_width), bf16),
            vmem((chosen.shape[1] * BLOCK_LENGTH, pair_width), bf16),
            vmem((rows, heads_width), bf16),
            vmem((half_rows, width), f32),
            vmem((half_rows, width), bf16),
            vmem((half_rows, width), bf16),
            dma,
            dma,
            dma,
            dma((2,)),
            dma((2,)),
            dma((4,)),
            dma((2 * (n_z - 1),)),
            dma((2 * (n_z - 1),)),
            dma((6 * n_z,)),
            dma((6 * n_z,)),
            dma((NEAR - 1,)),
            dma((NEAR - 1,)),
            dma((NEAR * n_y,)),
            dma((n_kv,)),
            dma((far * n_y,)),
            dma((far * n_y,)),
            dma((far * n_y,)),
            dma((2,)),
        ],
        compiler_params=pltpu.CompilerParams(
            collective_id=0, has_side_effects=True, vmem_limit_bytes=60 * 1024 * 1024
        ),
        name="fused",
    )(chosen, chosen, tokens, key_matrix, value_matrix, query_weight, out_weight.T)
    return (normed * out_gain[None, :]).astype(bf16)


def solution(mesh):
    n_dp, n_kv = mesh.shape["dp"], mesh.shape["kv"]
    n_y = 8
    placed = (
        P(("dp", "kv"), None),
        P(("dp", "kv"), None),
        P("kv", "tp"),
        P("kv", "tp"),
        P("kv", "tp"),
        P("tp", "kv"),
        P(),
    )
    return jax.shard_map(
        functools.partial(per_device, (n_dp, n_kv, n_y)),
        mesh=mesh,
        in_specs=placed,
        out_specs=P(("dp", "kv", "tp"), None),
        check_vma=False,
    )
```

```python
import functools

import jax
import jax.numpy as jnp
from jax import lax
from jax.experimental import pallas as pl
from jax.experimental.pallas import tpu as pltpu
from jax.sharding import PartitionSpec as P

HEAD_WIDTH = 64
BLOCK_LENGTH = 64
CAP = 2
NEAR = 5
NEG = -1e30
MESH = pl.DeviceIdType.MESH


def fused_kernel(
    dims,
    chosen_ref,
    chosen_rows,
    tokens_hbm,
    key_ref,
    value_ref,
    query_ref,
    out_ref,
    result_ref,
    placed_vmem,
    placed_ref,
    requests_ref,
    tokens,
    pair_all,
    requests_all,
    far_requests,
    requests_smem,
    query_all,
    out_all,
    own,
    chain1,
    chain2,
    chain3,
    chain4,
    pool,
    packed,
    far_packed,
    relayed,
    queries,
    gathered,
    gathered1,
    scores0,
    scores1,
    attended,
    part_mine,
    part_send,
    part_recv,
    tok_sem,
    place_sem,
    smem_sem,
    pair_sem,
    request_sem,
    y_sem,
    ring_send,
    ring_recv,
    x_send,
    x_recv,
    chain_send,
    chain_recv,
    block_send,
    block_recv,
    relay_send,
    relay_recv,
    onward_send,
    half_sem,
):
    n_dp, n_kv, n_y = dims
    n_z = n_kv // n_y
    dp, kv, tp = lax.axis_index("dp"), lax.axis_index("kv"), lax.axis_index("tp")
    z, y = kv // n_y, lax.rem(kv, n_y)
    depth = key_ref.shape[0]
    blocks = own.shape[0]
    quarter = query_ref.shape[1] // n_dp
    chains = (own, chain1, chain2, chain3, chain4)
    near = len(chains)
    n_far = n_z - near

    def remote(src, dst, send, recv, to_dp, to_kv, to_tp):
        return pltpu.make_async_remote_copy(
            src_ref=src,
            dst_ref=dst,
            send_sem=send,
            recv_sem=recv,
            device_id=(to_dp, to_kv, to_tp),
            device_id_type=MESH,
        )

    def drain(ref, sem):
        pltpu.make_async_copy(ref, ref, sem).wait()

    load_tokens = pltpu.make_async_copy(tokens_hbm, tokens, tok_sem)
    load_tokens.start()

    barrier = pltpu.get_barrier_semaphore()

    def row_mate(off):
        return z * n_y + lax.rem(y + off, n_y)

    def column_mate(off):
        return lax.rem(z + off, n_z) * n_y + y

    for off in range(1, n_y):
        pl.semaphore_signal(barrier, inc=1, device_id=(dp, row_mate(off), tp), device_id_type=MESH)
    for off in range(1, n_z):
        pl.semaphore_signal(
            barrier, inc=1, device_id=(dp, column_mate(off), tp), device_id_type=MESH
        )
    for off in range(1, n_dp):
        pl.semaphore_signal(
            barrier, inc=1, device_id=(lax.rem(dp + off, n_dp), kv, tp), device_id_type=MESH
        )
    pl.semaphore_signal(barrier, inc=1, device_id=(dp, kv, 1 - tp), device_id_type=MESH)

    my_rows = pl.ds(pl.multiple_of(kv * depth, depth), depth)
    my_cols = pl.ds(pl.multiple_of(dp * quarter, quarter), quarter)
    wide = jnp.float32
    pair = jnp.concatenate([key_ref[...].astype(wide), value_ref[...].astype(wide)], axis=1)
    pair_all[z, y] = pair.astype(jnp.bfloat16).reshape(pair_all.shape[2:])
    query_all[my_rows, my_cols] = query_ref[:, my_cols]
    out_all[my_rows, my_cols] = out_ref[:, my_cols]

    sel = chosen_ref.shape[1]
    table_lane = lax.broadcasted_iota(jnp.int32, (n_y, 128), 1)
    table_owner = lax.rem(z + n_z - lax.rem(table_lane // CAP, n_z), n_z) * n_y
    table_owner = table_owner + lax.broadcasted_iota(jnp.int32, (n_y, 128), 0)
    table_last = lax.rem(table_lane, CAP) > 0
    rows_at = chosen_rows[...]
    rows_owner = jnp.right_shift(rows_at, 3)

    def tabulate(at, carry):
        first, last, later = carry
        for s in range(sel):
            block = chosen_ref[at, s]
            owner = jnp.right_shift(block, 3)
            inner = jnp.bitwise_and(block, blocks - 1)
            mine = table_owner == owner
            first = jnp.where(mine, jnp.minimum(first, inner), first)
            last = jnp.where(mine, jnp.maximum(last, inner), last)
            later = jnp.where((rows_owner == owner) & (rows_at > block), 1, later)
        return first, last, later

    zeros = jnp.zeros((n_y, 128), jnp.int32)
    first, last, later = lax.fori_loop(
        0, blocks, tabulate, (zeros + (blocks - 1), zeros, jnp.zeros(rows_at.shape, jnp.int32))
    )
    requests_ref[...] = jnp.where(table_last, last, first).reshape(requests_ref.shape)
    steps_up = z - jnp.right_shift(rows_owner, 3)
    whole = (jnp.bitwise_and(rows_owner, n_y - 1) == y) & (steps_up < near)
    inside = n_kv * CAP + steps_up * blocks + jnp.bitwise_and(rows_at, blocks - 1)
    placed = jnp.where(whole, inside, rows_owner * CAP + later)
    placed_vmem[...] = jnp.zeros_like(placed_vmem)
    placed_vmem[:, :sel] = jnp.where(rows_at < 0, -1, placed)
    to_placed = pltpu.make_async_copy(placed_vmem, placed_ref, place_sem)
    to_placed.start()

    pl.semaphore_wait(barrier, n_y - 1 + n_z - 1 + n_dp - 1 + 1)

    def spread(piece, at, mate, count):
        def one(off, carry):
            remote(piece, piece, pair_sem.at[at], pair_sem.at[at + 1], dp, mate(off), tp).start()
            return carry

        lax.fori_loop(1, count, one, 0)

    spread(pair_all.at[z, y, 0], 0, row_mate, n_y)
    spread(pair_all.at[z, y, 1], 2, column_mate, n_z)

    def ask_row(off, carry):
        column = lax.rem(y + off, n_y)
        remote(
            requests_ref.at[pl.ds(column, 1)],
            requests_all.at[pl.ds(y, 1)],
            request_sem.at[0],
            request_sem.at[1],
            dp,
            row_mate(off),
            tp,
        ).start()
        return carry

    lax.fori_loop(1, n_y, ask_row, 0)
    for far in range(n_far):
        remote(
            requests_ref,
            far_requests.at[far],
            request_sem.at[2],
            request_sem.at[3],
            dp,
            column_mate(n_z - near - far),
            tp,
        ).start()

    def send_row(off, carry):
        for at, dst in enumerate((query_all, out_all)):
            remote(
                dst.at[my_rows, my_cols],
                dst.at[my_rows, my_cols],
                y_sem.at[2 * at],
                y_sem.at[2 * at + 1],
                dp,
                row_mate(off),
                tp,
            ).start()
        return carry

    lax.fori_loop(1, n_y, send_row, 0)

    pieces = pair_all.at[0, pl.ds(0, n_y - 1), 0]
    bundles = pair_all.at[pl.ds(0, n_z - 1), :, 0]
    drain(pieces, pair_sem.at[1])
    spread(pair_all.at[z, :, 0], 4, column_mate, n_z)
    drain(pieces, pair_sem.at[3])
    spread(pair_all.at[:, y, 1], 6, row_mate, n_y)

    near_asked = requests_all.at[pl.ds(0, n_y - 1)]
    far_asked = requests_all.at[pl.ds(0, n_far * n_y)]
    far_passed = requests_all.at[pl.ds(0, n_far * (n_y - 1))]
    drain(far_asked, request_sem.at[3])

    def pass_asked(off, carry):
        column = lax.rem(y + off, n_y)
        for far in range(n_far):
            remote(
                far_requests.at[far, pl.ds(column, 1)],
                requests_all.at[pl.ds(n_y * (1 + far) + y, 1)],
                request_sem.at[4],
                request_sem.at[5],
                dp,
                row_mate(off),
                tp,
            ).start()
        return carry

    lax.fori_loop(1, n_y, pass_asked, 0)
    for far in range(n_far):
        requests_all[n_y * (1 + far) + y] = far_requests[far, y]

    row_others = query_all.at[pl.ds(0, (n_y - 1) * depth), pl.ds(0, quarter)]

    above = lax.rem(z + 1, n_z) * n_y + y
    below = lax.rem(z + n_z - 1, n_z) * n_y + y
    right, left = lax.rem(dp + 1, n_dp), lax.rem(dp + n_dp - 1, n_dp)
    bundle_depth = n_y * depth
    downs = 2
    ups = n_z - 1 - downs

    def bundle(ref, delta, which):
        start = pl.multiple_of(lax.rem(z + n_z + delta, n_z) * bundle_depth, bundle_depth)
        cols = pl.multiple_of(lax.rem(dp + n_dp + which, n_dp) * quarter, quarter)
        return ref.at[pl.ds(start, bundle_depth), pl.ds(cols, quarter)]

    def ring(step, up):
        copies = []
        for part, ref in enumerate((query_all, out_all)):
            piece = bundle(ref, 1 - step if up else step - 1, 0)
            at = 2 * (step - 1 if up else ups + step - 1) + part
            copies.append(
                remote(
                    piece, piece, ring_send.at[at], ring_recv.at[at], dp, above if up else below, tp
                )
            )
        return copies

    def across(delta, kind):
        ref = out_all if kind in (2, 3, 5) else query_all
        which = {4: -1, 5: 1}.get(kind, 0)
        piece = bundle(ref, delta, which)
        at = lax.rem(z + n_z + delta, n_z) * 6 + kind
        to = right if kind in (0, 2, 4) else left
        return remote(piece, piece, x_send.at[at], x_recv.at[at], to, kv, tp)

    def cross(delta):
        for kind in range(4):
            across(delta, kind).start()

    def cross_on(delta):
        across(delta, 0).wait_recv()
        across(delta, 4).start()
        across(delta, 3).wait_recv()
        across(delta, 5).start()

    def start(copies):
        for copy in copies:
            copy.start()

    def arrive(copies):
        for copy in copies:
            copy.wait_recv()

    drain(row_others, y_sem.at[1])
    drain(row_others, y_sem.at[3])
    start(ring(1, True))
    start(ring(1, False))
    cross(0)
    arrive(ring(1, True))
    arrive(ring(1, False))
    start(ring(2, True))
    start(ring(2, False))
    cross(-1)
    cross(1)

    drain(near_asked, request_sem.at[1])
    drain(far_passed, request_sem.at[5])
    to_smem = pltpu.make_async_copy(requests_all, requests_smem, smem_sem)
    to_smem.start()
    load_tokens.wait()
    drain(bundles, pair_sem.at[5])
    drain(bundles, pair_sem.at[7])
    weights = pair_all[...].reshape(tokens.shape[1], own.shape[2])
    pairs = jnp.dot(tokens[...], weights, preferred_element_type=jnp.float32)
    pairs = pairs.astype(jnp.bfloat16).reshape(own.shape)
    own[...] = pairs
    pool[pl.ds(n_kv * CAP, blocks)] = pairs
    to_smem.wait()

    def climb(step):
        return remote(
            chains[step - 1],
            chains[step],
            chain_send.at[step - 1],
            chain_recv.at[step - 1],
            dp,
            above,
            tp,
        )

    def climb_on(step):
        @pl.when((z + 1 < n_z) & (z >= step - 1))
        def _():
            climb(step).start()

    def slots(owner):
        return pool.at[pl.ds(owner * CAP, CAP)]

    def far_copy(far, column):
        return remote(
            far_packed.at[far, column],
            relayed.at[far, y],
            relay_send.at[far * n_y + column],
            relay_recv.at[far * n_y + y],
            dp,
            z * n_y + column,
            tp,
        )

    def far_own(far):
        return remote(
            far_packed.at[far, y],
            slots(kv),
            relay_send.at[far * n_y + y],
            block_recv.at[kv],
            dp,
            (z + near + far) * n_y + y,
            tp,
        )

    def onward(far, column):
        owner = z * n_y + column
        return remote(
            relayed.at[far, column],
            slots(owner),
            onward_send.at[far * n_y + column],
            block_recv.at[owner],
            dp,
            (z + near + far) * n_y + y,
            tp,
        )

    def send_far(far):
        def one(off, carry):
            column = lax.rem(y + off, n_y)
            for slot in range(CAP):
                at = requests_smem[n_y * (1 + far) + column, 0, CAP * (near + far) + slot]
                far_packed[far, column, slot] = own[at]

            @pl.when(off > 0)
            def _():
                far_copy(far, column).start()

            @pl.when(off == 0)
            def _():
                far_own(far).start()

            return carry

        @pl.when(z + near + far < n_z)
        def _():
            lax.fori_loop(0, n_y, one, 0)

    def pass_far(far):
        def one(off, carry):
            column = lax.rem(y + off, n_y)
            relay = remote(
                far_packed.at[far, y],
                relayed.at[far, column],
                relay_send.at[far * n_y + y],
                relay_recv.at[far * n_y + column],
                dp,
                kv,
                tp,
            )
            relay.wait_recv()
            onward(far, column).start()
            return carry

        @pl.when(z + near + far < n_z)
        def _():
            lax.fori_loop(1, n_y, one, 0)

    def near_copy(step, column):
        owner = (z - step) * n_y + y
        return remote(
            packed.at[step, column],
            slots(owner),
            block_send.at[step * n_y + column],
            block_recv.at[owner],
            dp,
            z * n_y + column,
            tp,
        )

    def share(step):
        def one(off, carry):
            column = lax.rem(y + off, n_y)

            @pl.when((column > y) | (step > 0))
            def _():
                for slot in range(CAP):
                    at = requests_smem[column, 0, CAP * step + slot]
                    packed[step, column, slot] = chains[step][at]
                near_copy(step, column).start()

            return carry

        lax.fori_loop(1, n_y, one, 0)

    def take_chain(step):
        @pl.when(z >= step)
        def _():
            climb(step).wait_recv()

        if step + 1 < near:
            climb_on(step + 1)

        @pl.when(z >= step)
        def _():
            pool[pl.ds(n_kv * CAP + step * blocks, blocks)] = chains[step][...]
            share(step)

    climb_on(1)
    for far in reversed(range(n_far)):
        send_far(far)
    share(0)
    cross_on(0)

    arrive(ring(2, True))
    arrive(ring(2, False))
    start(ring(3, True))
    cross(-2)
    cross(2)
    pass_far(2)
    take_chain(1)
    cross_on(-1)
    cross_on(1)

    arrive(ring(3, True))
    start(ring(4, True))
    cross(-3)
    pass_far(1)
    take_chain(2)
    cross_on(-2)

    arrive(ring(4, True))
    start(ring(5, True))
    cross(-4)
    pass_far(0)
    take_chain(3)
    cross_on(2)
    cross_on(-3)

    arrive(ring(5, True))
    cross(-5)
    take_chain(4)
    cross_on(-4)
    cross_on(-5)

    def wait_across(kinds):
        def one(at, carry):
            for kind in kinds:
                across(at - z, kind).wait_recv()
            return carry

        lax.fori_loop(0, n_z, one, 0)

    wait_across((1, 4))

    lane = lax.broadcasted_iota(jnp.int32, (tokens.shape[0], 2 * HEAD_WIDTH), 1)
    for d in range(n_dp):
        rows = jnp.dot(
            tokens[...],
            query_all[:, d * quarter : (d + 1) * quarter],
            preferred_element_type=jnp.float32,
        )
        rows = rows.astype(jnp.bfloat16).astype(jnp.float32) * HEAD_WIDTH ** (-0.5)
        turned = pltpu.roll(rows, HEAD_WIDTH, 1)
        for side, value in enumerate((rows, turned)):
            head = jnp.where(lane < HEAD_WIDTH, value, 0.0).astype(jnp.bfloat16)
            queries[:, 2 * d + side] = head.reshape(blocks, BLOCK_LENGTH, 2 * HEAD_WIDTH)

    drain(pieces, pair_sem.at[0])
    drain(pieces, pair_sem.at[2])
    drain(bundles, pair_sem.at[4])
    drain(bundles, pair_sem.at[6])
    drain(near_asked, request_sem.at[0])
    drain(far_asked, request_sem.at[2])
    drain(far_passed, request_sem.at[4])
    drain(row_others, y_sem.at[0])
    drain(row_others, y_sem.at[2])
    for step in range(1, ups + 1):
        for copy in ring(step, True):
            copy.wait_send()
    for step in range(1, downs + 1):
        for copy in ring(step, False):
            copy.wait_send()

    for step in range(near):
        if step + 1 < near:

            @pl.when((z + 1 < n_z) & (z >= step))
            def _(step=step):
                climb(step + 1).wait_send()

        def drain_near(off, carry, step=step):
            column = lax.rem(y + off, n_y)

            @pl.when((z >= step) & ((column > y) | (step > 0)))
            def _():
                near_copy(step, column).wait_send()

            return carry

        lax.fori_loop(1, n_y, drain_near, 0)

    for far in range(n_far):

        def drain_far(off, carry, far=far):
            column = lax.rem(y + off, n_y)
            far_copy(far, column).wait_send()

            @pl.when(off > 0)
            def _():
                onward(far, column).wait_send()

            return carry

        @pl.when(z + near + far < n_z)
        def _(drain_far=drain_far):
            lax.fori_loop(0, n_y, drain_far, 0)

    def wait_blocks(owner, carry):
        steps = z - owner // n_y
        mate = lax.rem(owner, n_y)
        expected = (owner < kv) & ((steps == 0) | (steps >= near) | (mate != y))

        @pl.when(expected)
        def _():
            remote(
                packed.at[0, 0], slots(owner), block_send.at[0], block_recv.at[owner], dp, kv, tp
            ).wait_recv()

        return carry

    lax.fori_loop(0, n_kv, wait_blocks, 0)
    to_placed.wait()

    pair_rows = 2 * BLOCK_LENGTH
    row_at = lax.broadcasted_iota(jnp.int32, (pair_rows, 2 * HEAD_WIDTH), 0)
    lane_at = lax.broadcasted_iota(jnp.int32, (pair_rows, 2 * HEAD_WIDTH), 1)
    first_half = lane_at < BLOCK_LENGTH
    own_bias = jnp.where(lane_at <= lax.rem(row_at, BLOCK_LENGTH), 0.0, NEG)

    def gather(block, keys_ref):
        shut = []
        for s in range(sel):
            at = placed_ref[block, s]
            keys_ref[s * BLOCK_LENGTH : (s + 1) * BLOCK_LENGTH, :] = pool[jnp.maximum(at, 0)]
            shut.append(jnp.where(at < 0, NEG, 0.0))
        bias = [jnp.where(first_half, own_bias, shut[1])]
        for s in range(2, sel, 2):
            bias.append(jnp.where(first_half, shut[s], shut[s + 1]))
        return jnp.concatenate(bias, axis=1)

    def score(block, d, keys_ref, bias, scores_ref):
        query_pair = queries[block, 2 * d : 2 * d + 2].reshape(pair_rows, 2 * HEAD_WIDTH)
        scores = lax.dot_general(
            query_pair, keys_ref[...], (((1,), (1,)), ((), ())), preferred_element_type=jnp.float32
        )
        scores_ref[d] = scores + bias

    def soften(block, d, keys_ref, scores_ref):
        scores = scores_ref[d]
        expon = jnp.exp(scores - jnp.max(scores, axis=1, keepdims=True))
        total = jnp.sum(expon, axis=1, keepdims=True)
        mixed = jnp.dot(
            expon.astype(jnp.bfloat16), keys_ref[...], preferred_element_type=jnp.float32
        )
        mixed = mixed * (1.0 / total)
        even = pltpu.roll(mixed[:BLOCK_LENGTH], HEAD_WIDTH, 1)
        both = jnp.where(first_half[:BLOCK_LENGTH], even, mixed[BLOCK_LENGTH:])
        rows = pl.ds(pl.multiple_of(block * BLOCK_LENGTH, BLOCK_LENGTH), BLOCK_LENGTH)
        attended[rows, d * 2 * HEAD_WIDTH : (d + 1) * 2 * HEAD_WIDTH] = both.astype(jnp.bfloat16)

    def attend(pair, carry):
        block = 2 * pair
        ahead = jnp.minimum(block + 2, blocks - 1)
        bias = gather(block + 1, gathered1)
        for d in range(n_dp):
            score(block + 1, d, gathered1, bias, scores1)
            soften(block, d, gathered, scores0)
        bias = gather(ahead, gathered)
        for d in range(n_dp):
            score(ahead, d, gathered, bias, scores0)
            soften(block + 1, d, gathered1, scores1)
        return carry

    bias = gather(0, gathered)
    for d in range(n_dp):
        score(0, d, gathered, bias, scores0)
    lax.fori_loop(0, blocks // 2, attend, 0)

    wait_across((2, 5))

    def drain_across(at, carry):
        for kind in range(6):
            across(at - z, kind).wait_send()
        return carry

    lax.fori_loop(0, n_z, drain_across, 0)

    rows_out = part_mine.shape[0]

    def project(which):
        rows = attended[pl.ds(pl.multiple_of(which * rows_out, rows_out), rows_out), :]
        return lax.dot_general(
            rows, out_all[...], (((1,), (1,)), ((), ())), preferred_element_type=jnp.float32
        )

    part_send[...] = project(1 - tp).astype(jnp.bfloat16)
    swap = remote(part_send, part_recv, half_sem.at[0], half_sem.at[1], dp, kv, 1 - tp)
    swap.start()
    part_mine[...] = project(tp)
    swap.wait_recv()
    mixed = part_mine[...] + part_recv[...].astype(jnp.float32)
    scale = lax.rsqrt(jnp.mean(mixed * mixed, axis=1, keepdims=True) + 1e-06)
    result_ref[...] = mixed * scale

    swap.wait_send()


def per_device(dims, tokens, chosen, query_weight, key_matrix, value_matrix, out_weight, out_gain):
    n_dp, n_kv, n_y = dims
    rows, width = tokens.shape
    blocks = rows // BLOCK_LENGTH
    heads_width = query_weight.shape[1]
    pair_width = key_matrix.shape[1] + value_matrix.shape[1]
    half_rows = rows // 2
    n_z = n_kv // n_y
    far = n_z - NEAR
    vmem, dma = pltpu.VMEM, pltpu.SemaphoreType.DMA
    bf16, f32, i32 = jnp.bfloat16, jnp.float32, jnp.int32
    in_vmem = pl.BlockSpec(memory_space=pltpu.VMEM)
    normed = pl.pallas_call(
        functools.partial(fused_kernel, dims),
        out_shape=jax.ShapeDtypeStruct((half_rows, width), f32),
        in_specs=[
            pl.BlockSpec(memory_space=pltpu.SMEM),
            in_vmem,
            pl.BlockSpec(memory_space=pl.ANY),
            in_vmem,
            in_vmem,
            in_vmem,
            in_vmem,
        ],
        out_specs=in_vmem,
        scratch_shapes=[
            vmem((blocks, 128), i32),
            pltpu.SMEM((blocks, 128), i32),
            vmem((n_y, 1, 128), i32),
            vmem((rows, width), bf16),
            vmem((n_z, n_y, 2, key_matrix.shape[0] // 2, pair_width), bf16),
            vmem((n_y * (1 + far), 1, 128), i32),
            vmem((far, n_y, 1, 128), i32),
            pltpu.SMEM((n_y * (1 + far), 1, 128), i32),
            vmem((width, heads_width), bf16),
            vmem((width, heads_width), bf16),
            *[vmem((blocks, BLOCK_LENGTH, pair_width), bf16)] * NEAR,
            vmem((n_kv * CAP + NEAR * blocks, BLOCK_LENGTH, pair_width), bf16),
            vmem((NEAR, n_y, CAP, BLOCK_LENGTH, pair_width), bf16),
            vmem((far, n_y, CAP, BLOCK_LENGTH, pair_width), bf16),
            vmem((far, n_y, CAP, BLOCK_LENGTH, pair_width), bf16),
            vmem((blocks, heads_width // HEAD_WIDTH, BLOCK_LENGTH, pair_width), bf16),
            vmem((chosen.shape[1] * BLOCK_LENGTH, pair_width), bf16),
            vmem((chosen.shape[1] * BLOCK_LENGTH, pair_width), bf16),
            vmem((n_dp, 2 * BLOCK_LENGTH, chosen.shape[1] * BLOCK_LENGTH), f32),
            vmem((n_dp, 2 * BLOCK_LENGTH, chosen.shape[1] * BLOCK_LENGTH), f32),
            vmem((rows, heads_width), bf16),
            vmem((half_rows, width), f32),
            vmem((half_rows, width), bf16),
            vmem((half_rows, width), bf16),
            dma,
            dma,
            dma,
            dma((8,)),
            dma((6,)),
            dma((4,)),
            dma((2 * (n_z - 1),)),
            dma((2 * (n_z - 1),)),
            dma((6 * n_z,)),
            dma((6 * n_z,)),
            dma((NEAR - 1,)),
            dma((NEAR - 1,)),
            dma((NEAR * n_y,)),
            dma((n_kv,)),
            dma((far * n_y,)),
            dma((far * n_y,)),
            dma((far * n_y,)),
            dma((2,)),
        ],
        compiler_params=pltpu.CompilerParams(
            collective_id=0, has_side_effects=True, vmem_limit_bytes=60 * 1024 * 1024
        ),
        name="fused",
    )(chosen, chosen, tokens, key_matrix, value_matrix, query_weight, out_weight.T)
    return (normed * out_gain[None, :]).astype(bf16)


def solution(mesh):
    n_dp, n_kv = mesh.shape["dp"], mesh.shape["kv"]
    n_y = 8
    placed = (
        P(("dp", "kv"), None),
        P(("dp", "kv"), None),
        P("kv", "tp"),
        P("kv", "tp"),
        P("kv", "tp"),
        P("tp", "kv"),
        P(),
    )
    return jax.shard_map(
        functools.partial(per_device, (n_dp, n_kv, n_y)),
        mesh=mesh,
        in_specs=placed,
        out_specs=P(("dp", "kv", "tp"), None),
        check_vma=False,
    )
```

```python
import functools

import jax
import jax.numpy as jnp
from jax import lax
from jax.experimental import pallas as pl
from jax.experimental.pallas import tpu as pltpu
from jax.sharding import PartitionSpec as P

HEAD_WIDTH = 64
BLOCK_LENGTH = 64
CAP = 2
NEAR = 5
NEG = -1e30
MESH = pl.DeviceIdType.MESH


def fused_kernel(
    dims,
    chosen_ref,
    chosen_rows,
    tokens_hbm,
    key_ref,
    value_ref,
    query_ref,
    out_ref,
    result_ref,
    placed_vmem,
    placed_ref,
    requests_ref,
    tokens,
    pair_all,
    requests_all,
    far_requests,
    requests_smem,
    query_all,
    out_all,
    own,
    chain1,
    chain2,
    chain3,
    chain4,
    pool,
    packed,
    far_packed,
    relayed,
    queries,
    gathered,
    gathered1,
    scores0,
    scores1,
    attended,
    part_mine,
    part_send,
    part_recv,
    tok_sem,
    place_sem,
    smem_sem,
    pair_sem,
    request_sem,
    y_sem,
    ring_send,
    ring_recv,
    x_send,
    x_recv,
    chain_send,
    chain_recv,
    block_send,
    block_recv,
    relay_send,
    relay_recv,
    onward_send,
    half_sem,
):
    n_dp, n_kv, n_y = dims
    n_z = n_kv // n_y
    dp, kv, tp = lax.axis_index("dp"), lax.axis_index("kv"), lax.axis_index("tp")
    z, y = kv // n_y, lax.rem(kv, n_y)
    depth = key_ref.shape[0]
    blocks = own.shape[0]
    quarter = query_ref.shape[1] // n_dp
    chains = (own, chain1, chain2, chain3, chain4)
    near = len(chains)
    n_far = n_z - near

    def remote(src, dst, send, recv, to_dp, to_kv, to_tp):
        return pltpu.make_async_remote_copy(
            src_ref=src,
            dst_ref=dst,
            send_sem=send,
            recv_sem=recv,
            device_id=(to_dp, to_kv, to_tp),
            device_id_type=MESH,
        )

    def drain(ref, sem):
        pltpu.make_async_copy(ref, ref, sem).wait()

    load_tokens = pltpu.make_async_copy(tokens_hbm, tokens, tok_sem)
    load_tokens.start()

    barrier = pltpu.get_barrier_semaphore()

    def row_mate(off):
        return z * n_y + lax.rem(y + off, n_y)

    def column_mate(off):
        return lax.rem(z + off, n_z) * n_y + y

    for off in range(1, n_y):
        pl.semaphore_signal(barrier, inc=1, device_id=(dp, row_mate(off), tp), device_id_type=MESH)
    for off in range(1, n_z):
        pl.semaphore_signal(
            barrier, inc=1, device_id=(dp, column_mate(off), tp), device_id_type=MESH
        )
    for off in range(1, n_dp):
        pl.semaphore_signal(
            barrier, inc=1, device_id=(lax.rem(dp + off, n_dp), kv, tp), device_id_type=MESH
        )
    pl.semaphore_signal(barrier, inc=1, device_id=(dp, kv, 1 - tp), device_id_type=MESH)

    my_rows = pl.ds(pl.multiple_of(kv * depth, depth), depth)
    my_cols = pl.ds(pl.multiple_of(dp * quarter, quarter), quarter)
    wide = jnp.float32
    pair = jnp.concatenate([key_ref[...].astype(wide), value_ref[...].astype(wide)], axis=1)
    pair_all[z, y] = pair.astype(jnp.bfloat16).reshape(pair_all.shape[2:])
    query_all[my_rows, my_cols] = query_ref[:, my_cols]
    out_all[my_rows, my_cols] = out_ref[:, my_cols]

    sel = chosen_ref.shape[1]
    table_lane = lax.broadcasted_iota(jnp.int32, (n_y, 128), 1)
    table_owner = lax.rem(z + n_z - lax.rem(table_lane // CAP, n_z), n_z) * n_y
    table_owner = table_owner + lax.broadcasted_iota(jnp.int32, (n_y, 128), 0)
    table_last = lax.rem(table_lane, CAP) > 0
    rows_at = chosen_rows[...]
    rows_owner = jnp.right_shift(rows_at, 3)

    def tabulate(at, carry):
        first, last, later = carry
        for s in range(sel):
            block = chosen_ref[at, s]
            owner = jnp.right_shift(block, 3)
            inner = jnp.bitwise_and(block, blocks - 1)
            mine = table_owner == owner
            first = jnp.where(mine, jnp.minimum(first, inner), first)
            last = jnp.where(mine, jnp.maximum(last, inner), last)
            later = jnp.where((rows_owner == owner) & (rows_at > block), 1, later)
        return first, last, later

    zeros = jnp.zeros((n_y, 128), jnp.int32)
    first, last, later = lax.fori_loop(
        0, blocks, tabulate, (zeros + (blocks - 1), zeros, jnp.zeros(rows_at.shape, jnp.int32))
    )
    requests_ref[...] = jnp.where(table_last, last, first).reshape(requests_ref.shape)
    steps_up = z - jnp.right_shift(rows_owner, 3)
    whole = (jnp.bitwise_and(rows_owner, n_y - 1) == y) & (steps_up < near)
    inside = n_kv * CAP + steps_up * blocks + jnp.bitwise_and(rows_at, blocks - 1)
    placed = jnp.where(whole, inside, rows_owner * CAP + later)
    placed_vmem[...] = jnp.zeros_like(placed_vmem)
    placed_vmem[:, :sel] = jnp.where(rows_at < 0, -1, placed)
    to_placed = pltpu.make_async_copy(placed_vmem, placed_ref, place_sem)
    to_placed.start()

    pl.semaphore_wait(barrier, n_y - 1 + n_z - 1 + n_dp - 1 + 1)

    def spread(piece, at, mate, count):
        def one(off, carry):
            remote(piece, piece, pair_sem.at[at], pair_sem.at[at + 1], dp, mate(off), tp).start()
            return carry

        lax.fori_loop(1, count, one, 0)

    spread(pair_all.at[z, y, 0], 0, row_mate, n_y)
    spread(pair_all.at[z, y, 1], 2, column_mate, n_z)

    def ask_row(off, carry):
        column = lax.rem(y + off, n_y)
        remote(
            requests_ref.at[pl.ds(column, 1)],
            requests_all.at[pl.ds(y, 1)],
            request_sem.at[0],
            request_sem.at[1],
            dp,
            row_mate(off),
            tp,
        ).start()
        return carry

    lax.fori_loop(1, n_y, ask_row, 0)
    for far in range(n_far):
        remote(
            requests_ref,
            far_requests.at[far],
            request_sem.at[2],
            request_sem.at[3],
            dp,
            column_mate(n_z - near - far),
            tp,
        ).start()

    def send_row(off, carry):
        for at, dst in enumerate((query_all, out_all)):
            remote(
                dst.at[my_rows, my_cols],
                dst.at[my_rows, my_cols],
                y_sem.at[2 * at],
                y_sem.at[2 * at + 1],
                dp,
                row_mate(off),
                tp,
            ).start()
        return carry

    lax.fori_loop(1, n_y, send_row, 0)

    pieces = pair_all.at[0, pl.ds(0, n_y - 1), 0]
    bundles = pair_all.at[pl.ds(0, n_z - 1), :, 0]
    drain(pieces, pair_sem.at[1])
    spread(pair_all.at[z, :, 0], 4, column_mate, n_z)
    drain(pieces, pair_sem.at[3])
    spread(pair_all.at[:, y, 1], 6, row_mate, n_y)

    near_asked = requests_all.at[pl.ds(0, n_y - 1)]
    far_asked = requests_all.at[pl.ds(0, n_far * n_y)]
    far_passed = requests_all.at[pl.ds(0, n_far * (n_y - 1))]
    drain(far_asked, request_sem.at[3])

    def pass_asked(off, carry):
        column = lax.rem(y + off, n_y)
        for far in range(n_far):
            remote(
                far_requests.at[far, pl.ds(column, 1)],
                requests_all.at[pl.ds(n_y * (1 + far) + y, 1)],
                request_sem.at[4],
                request_sem.at[5],
                dp,
                row_mate(off),
                tp,
            ).start()
        return carry

    lax.fori_loop(1, n_y, pass_asked, 0)
    for far in range(n_far):
        requests_all[n_y * (1 + far) + y] = far_requests[far, y]

    row_others = query_all.at[pl.ds(0, (n_y - 1) * depth), pl.ds(0, quarter)]

    above = lax.rem(z + 1, n_z) * n_y + y
    below = lax.rem(z + n_z - 1, n_z) * n_y + y
    right, left = lax.rem(dp + 1, n_dp), lax.rem(dp + n_dp - 1, n_dp)
    bundle_depth = n_y * depth
    downs = 2
    ups = n_z - 1 - downs

    def bundle(ref, delta, which):
        start = pl.multiple_of(lax.rem(z + n_z + delta, n_z) * bundle_depth, bundle_depth)
        cols = pl.multiple_of(lax.rem(dp + n_dp + which, n_dp) * quarter, quarter)
        return ref.at[pl.ds(start, bundle_depth), pl.ds(cols, quarter)]

    def ring(step, up):
        copies = []
        for part, ref in enumerate((query_all, out_all)):
            piece = bundle(ref, 1 - step if up else step - 1, 0)
            at = 2 * (step - 1 if up else ups + step - 1) + part
            copies.append(
                remote(
                    piece, piece, ring_send.at[at], ring_recv.at[at], dp, above if up else below, tp
                )
            )
        return copies

    def across(delta, kind):
        ref = out_all if kind in (2, 3, 5) else query_all
        which = {4: -1, 5: 1}.get(kind, 0)
        piece = bundle(ref, delta, which)
        at = lax.rem(z + n_z + delta, n_z) * 6 + kind
        to = right if kind in (0, 2, 4) else left
        return remote(piece, piece, x_send.at[at], x_recv.at[at], to, kv, tp)

    def cross(part, *deltas):
        for delta in deltas:
            across(delta, 2 * part).start()
            across(delta, 2 * part + 1).start()

    def cross_on(part, *deltas):
        for delta in deltas:
            across(delta, 3 * part).wait_recv()
            across(delta, 4 + part).start()

    def start(copies):
        for copy in copies:
            copy.start()

    def arrive(copies):
        for copy in copies:
            copy.wait_recv()

    drain(row_others, y_sem.at[1])
    drain(row_others, y_sem.at[3])
    start(ring(1, True))
    start(ring(1, False))
    cross(0, 0)
    cross(1, 0)
    arrive(ring(1, True))
    arrive(ring(1, False))
    start(ring(2, True))
    start(ring(2, False))
    cross(0, -1, 1)
    cross_on(0, 0)

    drain(near_asked, request_sem.at[1])
    drain(far_passed, request_sem.at[5])
    to_smem = pltpu.make_async_copy(requests_all, requests_smem, smem_sem)
    to_smem.start()
    load_tokens.wait()
    drain(bundles, pair_sem.at[5])
    drain(bundles, pair_sem.at[7])
    weights = pair_all[...].reshape(tokens.shape[1], own.shape[2])
    pairs = jnp.dot(tokens[...], weights, preferred_element_type=jnp.float32)
    pairs = pairs.astype(jnp.bfloat16).reshape(own.shape)
    own[...] = pairs
    pool[pl.ds(n_kv * CAP, blocks)] = pairs
    to_smem.wait()

    def climb(step):
        return remote(
            chains[step - 1],
            chains[step],
            chain_send.at[step - 1],
            chain_recv.at[step - 1],
            dp,
            above,
            tp,
        )

    def climb_on(step):
        @pl.when((z + 1 < n_z) & (z >= step - 1))
        def _():
            climb(step).start()

    def slots(owner):
        return pool.at[pl.ds(owner * CAP, CAP)]

    def far_copy(far, column):
        return remote(
            far_packed.at[far, column],
            relayed.at[far, y],
            relay_send.at[far * n_y + column],
            relay_recv.at[far * n_y + y],
            dp,
            z * n_y + column,
            tp,
        )

    def far_own(far):
        return remote(
            far_packed.at[far, y],
            slots(kv),
            relay_send.at[far * n_y + y],
            block_recv.at[kv],
            dp,
            (z + near + far) * n_y + y,
            tp,
        )

    def onward(far, column):
        owner = z * n_y + column
        return remote(
            relayed.at[far, column],
            slots(owner),
            onward_send.at[far * n_y + column],
            block_recv.at[owner],
            dp,
            (z + near + far) * n_y + y,
            tp,
        )

    def send_far(far):
        def one(off, carry):
            column = lax.rem(y + off, n_y)
            for slot in range(CAP):
                at = requests_smem[n_y * (1 + far) + column, 0, CAP * (near + far) + slot]
                far_packed[far, column, slot] = own[at]

            @pl.when(off > 0)
            def _():
                far_copy(far, column).start()

            @pl.when(off == 0)
            def _():
                far_own(far).start()

            return carry

        @pl.when(z + near + far < n_z)
        def _():
            lax.fori_loop(0, n_y, one, 0)

    def pass_far(far):
        def one(off, carry):
            column = lax.rem(y + off, n_y)
            relay = remote(
                far_packed.at[far, y],
                relayed.at[far, column],
                relay_send.at[far * n_y + y],
                relay_recv.at[far * n_y + column],
                dp,
                kv,
                tp,
            )
            relay.wait_recv()
            onward(far, column).start()
            return carry

        @pl.when(z + near + far < n_z)
        def _():
            lax.fori_loop(1, n_y, one, 0)

    def near_copy(step, column):
        owner = (z - step) * n_y + y
        return remote(
            packed.at[step, column],
            slots(owner),
            block_send.at[step * n_y + column],
            block_recv.at[owner],
            dp,
            z * n_y + column,
            tp,
        )

    def share(step):
        def one(off, carry):
            column = lax.rem(y + off, n_y)

            @pl.when((column > y) | (step > 0))
            def _():
                for slot in range(CAP):
                    at = requests_smem[column, 0, CAP * step + slot]
                    packed[step, column, slot] = chains[step][at]
                near_copy(step, column).start()

            return carry

        lax.fori_loop(1, n_y, one, 0)

    def take_chain(step):
        @pl.when(z >= step)
        def _():
            climb(step).wait_recv()

        if step + 1 < near:
            climb_on(step + 1)

        @pl.when(z >= step)
        def _():
            pool[pl.ds(n_kv * CAP + step * blocks, blocks)] = chains[step][...]
            share(step)

    climb_on(1)
    for far in reversed(range(n_far)):
        send_far(far)
    share(0)

    arrive(ring(2, True))
    arrive(ring(2, False))
    start(ring(3, True))
    cross(0, -2, 2)
    cross_on(0, -1, 1)
    cross(1, -1, 1)
    pass_far(2)
    take_chain(1)
    cross_on(1, 0)

    arrive(ring(3, True))
    start(ring(4, True))
    cross(0, -3)
    cross_on(0, -2, 2)
    cross(1, -2, 2)
    pass_far(1)
    take_chain(2)
    cross_on(1, -1, 1)

    arrive(ring(4, True))
    start(ring(5, True))
    cross(0, -4)
    cross_on(0, -3)
    cross(1, -3)
    pass_far(0)
    take_chain(3)
    cross_on(1, -2, 2)

    arrive(ring(5, True))
    cross(0, -5)
    cross_on(0, -4)
    cross(1, -4)
    take_chain(4)
    cross_on(0, -5)
    cross(1, -5)

    def wait_across(kinds):
        def one(at, carry):
            for kind in kinds:
                across(at - z, kind).wait_recv()
            return carry

        lax.fori_loop(0, n_z, one, 0)

    wait_across((1, 4))

    lane = lax.broadcasted_iota(jnp.int32, (tokens.shape[0], 2 * HEAD_WIDTH), 1)
    for d in range(n_dp):
        rows = jnp.dot(
            tokens[...],
            query_all[:, d * quarter : (d + 1) * quarter],
            preferred_element_type=jnp.float32,
        )
        rows = rows.astype(jnp.bfloat16).astype(jnp.float32) * HEAD_WIDTH ** (-0.5)
        turned = pltpu.roll(rows, HEAD_WIDTH, 1)
        for side, value in enumerate((rows, turned)):
            head = jnp.where(lane < HEAD_WIDTH, value, 0.0).astype(jnp.bfloat16)
            queries[:, 2 * d + side] = head.reshape(blocks, BLOCK_LENGTH, 2 * HEAD_WIDTH)

    cross_on(1, -3, -4, -5)
    drain(pieces, pair_sem.at[0])
    drain(pieces, pair_sem.at[2])
    drain(bundles, pair_sem.at[4])
    drain(bundles, pair_sem.at[6])
    drain(near_asked, request_sem.at[0])
    drain(far_asked, request_sem.at[2])
    drain(far_passed, request_sem.at[4])
    drain(row_others, y_sem.at[0])
    drain(row_others, y_sem.at[2])
    for step in range(1, ups + 1):
        for copy in ring(step, True):
            copy.wait_send()
    for step in range(1, downs + 1):
        for copy in ring(step, False):
            copy.wait_send()

    for step in range(near):
        if step + 1 < near:

            @pl.when((z + 1 < n_z) & (z >= step))
            def _(step=step):
                climb(step + 1).wait_send()

        def drain_near(off, carry, step=step):
            column = lax.rem(y + off, n_y)

            @pl.when((z >= step) & ((column > y) | (step > 0)))
            def _():
                near_copy(step, column).wait_send()

            return carry

        lax.fori_loop(1, n_y, drain_near, 0)

    for far in range(n_far):

        def drain_far(off, carry, far=far):
            column = lax.rem(y + off, n_y)
            far_copy(far, column).wait_send()

            @pl.when(off > 0)
            def _():
                onward(far, column).wait_send()

            return carry

        @pl.when(z + near + far < n_z)
        def _(drain_far=drain_far):
            lax.fori_loop(0, n_y, drain_far, 0)

    def wait_blocks(owner, carry):
        steps = z - owner // n_y
        mate = lax.rem(owner, n_y)
        expected = (owner < kv) & ((steps == 0) | (steps >= near) | (mate != y))

        @pl.when(expected)
        def _():
            remote(
                packed.at[0, 0], slots(owner), block_send.at[0], block_recv.at[owner], dp, kv, tp
            ).wait_recv()

        return carry

    lax.fori_loop(0, n_kv, wait_blocks, 0)
    to_placed.wait()

    pair_rows = 2 * BLOCK_LENGTH
    row_at = lax.broadcasted_iota(jnp.int32, (pair_rows, 2 * HEAD_WIDTH), 0)
    lane_at = lax.broadcasted_iota(jnp.int32, (pair_rows, 2 * HEAD_WIDTH), 1)
    first_half = lane_at < BLOCK_LENGTH
    own_bias = jnp.where(lane_at <= lax.rem(row_at, BLOCK_LENGTH), 0.0, NEG)

    def gather(block, keys_ref):
        shut = []
        for s in range(sel):
            at = placed_ref[block, s]
            keys_ref[s * BLOCK_LENGTH : (s + 1) * BLOCK_LENGTH, :] = pool[jnp.maximum(at, 0)]
            shut.append(jnp.where(at < 0, NEG, 0.0))
        bias = [jnp.where(first_half, own_bias, shut[1])]
        for s in range(2, sel, 2):
            bias.append(jnp.where(first_half, shut[s], shut[s + 1]))
        return jnp.concatenate(bias, axis=1)

    def score(block, d, keys_ref, bias, scores_ref):
        query_pair = queries[block, 2 * d : 2 * d + 2].reshape(pair_rows, 2 * HEAD_WIDTH)
        scores = lax.dot_general(
            query_pair, keys_ref[...], (((1,), (1,)), ((), ())), preferred_element_type=jnp.float32
        )
        scores_ref[d] = scores + bias

    def soften(block, d, keys_ref, scores_ref):
        scores = scores_ref[d]
        expon = jnp.exp(scores - jnp.max(scores, axis=1, keepdims=True))
        total = jnp.sum(expon, axis=1, keepdims=True)
        mixed = jnp.dot(
            expon.astype(jnp.bfloat16), keys_ref[...], preferred_element_type=jnp.float32
        )
        mixed = mixed * (1.0 / total)
        even = pltpu.roll(mixed[:BLOCK_LENGTH], HEAD_WIDTH, 1)
        both = jnp.where(first_half[:BLOCK_LENGTH], even, mixed[BLOCK_LENGTH:])
        rows = pl.ds(pl.multiple_of(block * BLOCK_LENGTH, BLOCK_LENGTH), BLOCK_LENGTH)
        attended[rows, d * 2 * HEAD_WIDTH : (d + 1) * 2 * HEAD_WIDTH] = both.astype(jnp.bfloat16)

    def turn(at):
        return lax.rem(at + (1 - tp) * (blocks // 2), blocks)

    def attend(pair, carry):
        block, after = turn(2 * pair), turn(2 * pair + 1)
        ahead = turn(jnp.minimum(2 * pair + 2, blocks - 1))
        bias = gather(after, gathered1)
        for d in range(n_dp):
            score(after, d, gathered1, bias, scores1)
            soften(block, d, gathered, scores0)
        bias = gather(ahead, gathered)
        for d in range(n_dp):
            score(ahead, d, gathered, bias, scores0)
            soften(after, d, gathered1, scores1)
        return carry

    bias = gather(turn(0), gathered)
    for d in range(n_dp):
        score(turn(0), d, gathered, bias, scores0)
    lax.fori_loop(0, blocks // 4, attend, 0)

    wait_across((2, 5))

    rows_out = part_mine.shape[0]

    def project(which):
        rows = attended[pl.ds(pl.multiple_of(which * rows_out, rows_out), rows_out), :]
        return lax.dot_general(
            rows, out_all[...], (((1,), (1,)), ((), ())), preferred_element_type=jnp.float32
        )

    part_send[...] = project(1 - tp).astype(jnp.bfloat16)
    swap = remote(part_send, part_recv, half_sem.at[0], half_sem.at[1], dp, kv, 1 - tp)
    swap.start()
    lax.fori_loop(blocks // 4, blocks // 2, attend, 0)
    def drain_across(at, carry):
        for kind in range(6):
            across(at - z, kind).wait_send()
        return carry

    lax.fori_loop(0, n_z, drain_across, 0)
    part_mine[...] = project(tp)
    swap.wait_recv()
    mixed = part_mine[...] + part_recv[...].astype(jnp.float32)
    scale = lax.rsqrt(jnp.mean(mixed * mixed, axis=1, keepdims=True) + 1e-06)
    result_ref[...] = mixed * scale

    swap.wait_send()


def per_device(dims, tokens, chosen, query_weight, key_matrix, value_matrix, out_weight, out_gain):
    n_dp, n_kv, n_y = dims
    rows, width = tokens.shape
    blocks = rows // BLOCK_LENGTH
    heads_width = query_weight.shape[1]
    pair_width = key_matrix.shape[1] + value_matrix.shape[1]
    half_rows = rows // 2
    n_z = n_kv // n_y
    far = n_z - NEAR
    vmem, dma = pltpu.VMEM, pltpu.SemaphoreType.DMA
    bf16, f32, i32 = jnp.bfloat16, jnp.float32, jnp.int32
    in_vmem = pl.BlockSpec(memory_space=pltpu.VMEM)
    normed = pl.pallas_call(
        functools.partial(fused_kernel, dims),
        out_shape=jax.ShapeDtypeStruct((half_rows, width), f32),
        in_specs=[
            pl.BlockSpec(memory_space=pltpu.SMEM),
            in_vmem,
            pl.BlockSpec(memory_space=pl.ANY),
            in_vmem,
            in_vmem,
            in_vmem,
            in_vmem,
        ],
        out_specs=in_vmem,
        scratch_shapes=[
            vmem((blocks, 128), i32),
            pltpu.SMEM((blocks, 128), i32),
            vmem((n_y, 1, 128), i32),
            vmem((rows, width), bf16),
            vmem((n_z, n_y, 2, key_matrix.shape[0] // 2, pair_width), bf16),
            vmem((n_y * (1 + far), 1, 128), i32),
            vmem((far, n_y, 1, 128), i32),
            pltpu.SMEM((n_y * (1 + far), 1, 128), i32),
            vmem((width, heads_width), bf16),
            vmem((width, heads_width), bf16),
            *[vmem((blocks, BLOCK_LENGTH, pair_width), bf16)] * NEAR,
            vmem((n_kv * CAP + NEAR * blocks, BLOCK_LENGTH, pair_width), bf16),
            vmem((NEAR, n_y, CAP, BLOCK_LENGTH, pair_width), bf16),
            vmem((far, n_y, CAP, BLOCK_LENGTH, pair_width), bf16),
            vmem((far, n_y, CAP, BLOCK_LENGTH, pair_width), bf16),
            vmem((blocks, heads_width // HEAD_WIDTH, BLOCK_LENGTH, pair_width), bf16),
            vmem((chosen.shape[1] * BLOCK_LENGTH, pair_width), bf16),
            vmem((chosen.shape[1] * BLOCK_LENGTH, pair_width), bf16),
            vmem((n_dp, 2 * BLOCK_LENGTH, chosen.shape[1] * BLOCK_LENGTH), f32),
            vmem((n_dp, 2 * BLOCK_LENGTH, chosen.shape[1] * BLOCK_LENGTH), f32),
            vmem((rows, heads_width), bf16),
            vmem((half_rows, width), f32),
            vmem((half_rows, width), bf16),
            vmem((half_rows, width), bf16),
            dma,
            dma,
            dma,
            dma((8,)),
            dma((6,)),
            dma((4,)),
            dma((2 * (n_z - 1),)),
            dma((2 * (n_z - 1),)),
            dma((6 * n_z,)),
            dma((6 * n_z,)),
            dma((NEAR - 1,)),
            dma((NEAR - 1,)),
            dma((NEAR * n_y,)),
            dma((n_kv,)),
            dma((far * n_y,)),
            dma((far * n_y,)),
            dma((far * n_y,)),
            dma((2,)),
        ],
        compiler_params=pltpu.CompilerParams(
            collective_id=0, has_side_effects=True, vmem_limit_bytes=60 * 1024 * 1024
        ),
        name="fused",
    )(chosen, chosen, tokens, key_matrix, value_matrix, query_weight, out_weight.T)
    return (normed * out_gain[None, :]).astype(bf16)


def solution(mesh):
    n_dp, n_kv = mesh.shape["dp"], mesh.shape["kv"]
    n_y = 8
    placed = (
        P(("dp", "kv"), None),
        P(("dp", "kv"), None),
        P("kv", "tp"),
        P("kv", "tp"),
        P("kv", "tp"),
        P("tp", "kv"),
        P(),
    )
    return jax.shard_map(
        functools.partial(per_device, (n_dp, n_kv, n_y)),
        mesh=mesh,
        in_specs=placed,
        out_specs=P(("dp", "kv", "tp"), None),
        check_vma=False,
    )
```
